256 devices in a mesh: grp: 4 (over y, x), ep: 64 (over z, core).
Axes of the slice: x: 2, y: 2, z: 32, core: 2. Of those that a mesh axis runs over, the one named last changes fastest.
The devices are a block of a 4x8x32 slice.
Arguments:
- tokens: bfloat16 [2048, 2048], P(('grp', 'ep')), parts along dimension 0, may hold values from -6 to 6
- routes: int32 [2048, 4], P(('grp', 'ep')), parts along dimension 0, may hold values from 0 to 63, all different within a row; in each aligned block of 8 rows (0 to 7, 8 to 15, ...) at most 2 rows name the same one
- gate_weights: float32 [2048, 4], P(('grp', 'ep')), parts along dimension 0, may hold values from 0.1 to 1
- norm_gain: float32 [2048], replicated, may hold values from 0.1 to 1.9
- final_gain: float32 [2048], replicated, may hold values from 0.1 to 1.9
- w_gate: bfloat16 [64, 2048, 512], P('ep'), may hold values from -0.088388348 to 0.088388348
- w_up: bfloat16 [64, 2048, 512], P('ep'), may hold values from -0.088388348 to 0.088388348
- w_down: bfloat16 [64, 512, 2048], P('ep'), may hold values from -0.176776695 to 0.176776695
Outputs:
- mixed: bfloat16 [2048, 2048], P('grp', 'ep'), parts along dimension 0
The draws below stay inside these ranges and needn't reach their ends.
There are 4 independent parts, one for each index of `grp`. The reference program is written for one: setup_inputs(seed, part) draws one part's arguments, and reference() takes and returns one part's arrays. A program takes and returns all parts, laid end to end along the dimension named above; an argument that names none is the same for every part. Nothing has to cross between parts.
Inputs may be any that keep to these rules, and one draw needn't show every extreme that they name: `routes`: each row names 4 different experts; among the rows of one device no expert is named by more than 2 rows, and some expert reaches 2.
All inputs are finite; a program needn't handle non-finite values.
Results may differ from the reference program's by a relative error of at most 0.008.
Values may be sent and summed in bfloat16 or wider, within the bound.
No kernel may reach another device: no remote copies, remote signals or barrier semaphores. Data moves between devices by JAX's collectives and lax.ppermute only.
A program may use at most 64 MiB of HBM per device.

```python
import math
import jax
import jax.numpy as jnp
import numpy as np
from jax import lax

D = 2048
FF_E = 512
TOPK = 4
TOK_DEV = 8
MOST = 2
EXPERTS = 64
TOKENS = 512
N_EP = 64


def shared_experts(key, salt, rows, cols):
    share = 0.5
    common = jax.random.normal(jax.random.fold_in(key, salt), (rows, cols), jnp.float32)
    own = jax.random.normal(jax.random.fold_in(key, salt + 1), (EXPERTS, rows, cols), jnp.float32)
    mixture = math.sqrt(share) * common[None] + math.sqrt(1.0 - share) * own
    return (jnp.clip(mixture, -4.0, 4.0) * rows ** (-0.5)).astype(jnp.bfloat16)


def draw_w_gate(key, part):
    return shared_experts(key, 101, D, FF_E)


def draw_w_up(key, part):
    return shared_experts(key, 203, D, FF_E)


def draw_w_down(key, part):
    return shared_experts(key, 307, FF_E, D)


def level_of(stream_key, dims, split, smallest, top_value):
    def one(axis_at, shards_of):
        heights = jax.random.uniform(jax.random.fold_in(jax.random.fold_in(stream_key, 6), axis_at), (shards_of,), jnp.float32, smallest / len(split), top_value / len(split))
        return jnp.repeat(jnp.exp(heights), dims[axis_at] // shards_of).reshape((-1,) + (1,) * (len(dims) - axis_at - 1))

    factor_of = one(*split[0])
    for cut in split[1:]:
        factor_of = factor_of * one(*cut)
    return factor_of


def deal_out(key, own, number, rows, number_of, top, bound, slope):
    order = jax.random.permutation(key, number_of)
    heavy_load, ordinary = portions_of(number_of, rows * top, bound, slope, True), portions_of(number_of, rows * top, bound, slope, False)
    places = jnp.arange(number_of)

    def named(sizes, offset_by):
        used = int((sizes > 0).sum())
        fixed = max(1, used // 4)
        moved = fixed + (places - fixed + offset_by * (used - fixed)) % max(1, number_of - fixed)
        return jnp.zeros((number_of,), jnp.int32).at[order[jnp.where(places < fixed, places, moved)]].set(jnp.asarray(sizes, jnp.int32))

    sizes = jnp.where(number % 4 == 0, named(heavy_load, number // 4), named(ordinary, number - number // 4 - 1))
    mixed = jax.random.permutation(jax.random.fold_in(own, 3), number_of)
    source_of, sink = mixed[0:number_of // 2 * 2:2], mixed[1:number_of // 2 * 2:2]
    margin = jnp.minimum(sizes[source_of] - 1, bound - sizes[sink]) // 2
    margin = jnp.where((source_of == order[0]) | (sink == order[0]) | (sizes[sink] == 0), 0, jnp.maximum(margin, 0))
    moved = jax.random.randint(jax.random.fold_in(own, 4), (number_of // 2,), 0, 1 << 20) % (margin + 1)
    sizes = sizes.at[source_of].add(-moved).at[sink].add(moved)
    members = jnp.searchsorted(jnp.cumsum(sizes), jnp.arange(rows * top), side="right").astype(jnp.int32)
    table = members.reshape(top, rows).T
    table = table[jax.random.permutation(jax.random.fold_in(own, 1), rows)]
    offset_by = jax.random.randint(jax.random.fold_in(own, 2), (rows, 1), 0, top)
    return jnp.take_along_axis(table, (jnp.arange(top)[None, :] + offset_by) % top, axis=1)


def portions_of(count, total, bound, slope, full):
    portions = [(1 << 20) // math.isqrt(grade ** slope) + 1 for grade in range(1, count + 1)]
    largest = bound if full else min(bound, max(-(-total // count), total * portions[0] // sum(portions)))
    least = 1 if total - largest >= count - 1 else 0
    holding, surplus = [largest] + [least] * (count - 1), total - largest - least * (count - 1)
    while surplus > 0:
        candidates = [i for i in range(1, count) if holding[i] < largest] or [i for i in range(1, count) if holding[i] < bound]
        mass, left = sum([portions[i] for i in candidates]), surplus
        for i in candidates:
            extra = min(bound - holding[i], max(1, left * portions[i] // mass), surplus)
            holding[i] = holding[i] + extra
            surplus = surplus - extra
    return np.array(holding)


def scatter_about(rng, dims, scale, reach, shards=(), held_as=jnp.bfloat16):
    drawn = scale * jax.random.normal(rng, dims, jnp.float32)
    if shards:
        drawn = drawn * level_of(rng, dims, shards, -0.22, 0.18)
    return jnp.clip(drawn, -reach, reach).astype(held_as)


def setup_inputs(seed: int = 0, part: int = 0) -> dict:
    arg_keys = jax.random.split(jax.random.key(seed), 9)
    own_keys = jax.random.split(jax.random.fold_in(arg_keys[8], part), 9)
    tokens = scatter_about(own_keys[0], (TOKENS, D), 1.0, 6.0, ((0, 64),))
    routes_keys = jax.random.split(jax.random.fold_in(own_keys[1], 1), TOKENS // TOK_DEV)
    routes_turns = jax.random.permutation(jax.random.fold_in(own_keys[1], 3), TOKENS // TOK_DEV)
    routes = jax.vmap(lambda own, number: deal_out(jax.random.fold_in(own_keys[1], 2), own, number, TOK_DEV, EXPERTS, TOPK, MOST, 2))(routes_keys, routes_turns).reshape((TOKENS, TOPK))
    gate_weights = jnp.clip(0.1 + 0.9 * jax.random.uniform(own_keys[2], (TOKENS, TOPK), jnp.float32) ** level_of(own_keys[2], (TOKENS, TOPK), ((0, 64),), -0.2, 0.2), 0.1, 1.0)
    norm_gain = jnp.clip(1.0 + 0.18 * jax.random.normal(arg_keys[3], (D,), jnp.float32), 0.1, 1.9)
    final_gain = jnp.clip(1.0 + 0.18 * jax.random.normal(arg_keys[4], (D,), jnp.float32), 0.1, 1.9)
    w_gate = draw_w_gate(jax.random.fold_in(arg_keys[8], 71), part)
    w_up = draw_w_up(jax.random.fold_in(arg_keys[8], 71), part)
    w_down = draw_w_down(jax.random.fold_in(arg_keys[8], 71), part)
    return dict(tokens=tokens, routes=routes, gate_weights=gate_weights, norm_gain=norm_gain, final_gain=final_gain, w_gate=w_gate, w_up=w_up, w_down=w_down)


def reference(tokens, routes, gate_weights, norm_gain, final_gain, w_gate, w_up, w_down):
    epsilon = 1e-06
    values = tokens.astype(jnp.float32)
    normed = (values * lax.rsqrt(lax.optimization_barrier(jnp.mean(values * values, axis=1, keepdims=True)) + epsilon) * norm_gain).astype(jnp.bfloat16)
    capacity = min(TOKENS, N_EP * MOST)
    normed_wide = normed.astype(jnp.float32)

    def one_expert(carry, expert):
        match = (routes == expert).astype(jnp.float32)
        weight_row = lax.optimization_barrier(jnp.sum(match * gate_weights, axis=1))
        used = lax.optimization_barrier(jnp.sum(match, axis=1)).astype(jnp.int32)
        picked = jnp.argsort(1 - used, stable=True)[:capacity].astype(jnp.int32)
        rows = normed_wide[picked]
        gate_mat = lax.dynamic_index_in_dim(w_gate, expert, 0, keepdims=False).astype(jnp.float32)
        up_mat = lax.dynamic_index_in_dim(w_up, expert, 0, keepdims=False).astype(jnp.float32)
        down_mat = lax.dynamic_index_in_dim(w_down, expert, 0, keepdims=False).astype(jnp.float32)
        gate_val = jnp.dot(rows, gate_mat, preferred_element_type=jnp.float32)
        up_val = jnp.dot(rows, up_mat, preferred_element_type=jnp.float32)
        act = (jax.nn.silu(gate_val) * up_val).astype(jnp.bfloat16).astype(jnp.float32)
        result = jnp.dot(act, down_mat, preferred_element_type=jnp.float32).astype(jnp.bfloat16)
        carry = carry.at[picked].add(weight_row[picked][:, None] * result.astype(jnp.float32))
        return (carry, 0)
    start = jnp.zeros((TOKENS, D), jnp.float32)
    combined, unused = lax.scan(one_expert, start, jnp.arange(EXPERTS, dtype=jnp.int32))
    scale = lax.rsqrt(lax.optimization_barrier(jnp.mean(combined * combined, axis=1, keepdims=True)) + epsilon)
    return (combined * scale * final_gain).astype(jnp.bfloat16)
```

```python
import jax
import jax.numpy as jnp
from jax import lax
from jax.experimental import pallas as pl
from jax.experimental.pallas import tpu as pltpu
from jax.sharding import Mesh
from jax.sharding import PartitionSpec as P

EP = ("zh", "zl", "core")
GRP_EP = ("grp", "zh", "zl", "core")
LANES = 128


def swapped(parts, flag_low, flag_high):
    a, b, c, d = parts
    a, b, c, d = (
        jnp.where(flag_low, b, a),
        jnp.where(flag_low, a, b),
        jnp.where(flag_low, d, c),
        jnp.where(flag_low, c, d),
    )
    return (
        jnp.where(flag_high, c, a),
        jnp.where(flag_high, d, b),
        jnp.where(flag_high, a, c),
        jnp.where(flag_high, b, d),
    )


def combine_kernel(rows_ref, src_ref, lane_ref, out_ref):
    devices, cols, slots = rows_ref.shape
    tokens = src_ref.shape[1]
    topk = src_ref.shape[0]
    slot = lax.broadcasted_iota(jnp.int32, (slots, tokens), 0)
    src = src_ref[...]
    lane = lane_ref[...]

    def step(s, acc):
        key = jnp.where(src == s, lane, -1)
        hit = slot == key[0:1, :]
        for k in range(1, topk):
            hit = hit | (slot == key[k : k + 1, :])
        pick = jnp.where(hit, 1.0, 0.0).astype(jnp.bfloat16)
        return acc + jnp.dot(rows_ref[s], pick, preferred_element_type=jnp.float32)

    out_ref[...] = lax.fori_loop(
        0, devices, step, jnp.zeros((cols, tokens), jnp.float32), unroll=4
    )


def combine(rows, src, lane):
    return pl.pallas_call(
        combine_kernel,
        out_shape=jax.ShapeDtypeStruct((rows.shape[1], src.shape[1]), jnp.float32),
    )(rows, src, lane)


def shards(tokens, routes, gate_weights, norm_gain, final_gain, w_gate, w_up, w_down):
    epsilon = 1e-06
    per_dev, width = tokens.shape
    topk = routes.shape[1]
    group = lax.axis_size(EP)
    cols = width // group
    total = per_dev * group
    most = 2 * group
    me = lax.axis_index(EP)
    core = lax.axis_index("core")
    odd = lax.axis_index("zl")

    values = tokens.astype(jnp.float32)
    normed = (
        values * lax.rsqrt(jnp.mean(values * values, axis=1, keepdims=True) + epsilon) * norm_gain
    ).astype(jnp.bfloat16)
    high = lax.reduce_precision(gate_weights, 8, 7)
    rest = gate_weights - high
    mid = lax.reduce_precision(rest, 8, 7)
    low = rest - mid
    meta = jnp.concatenate([routes.astype(jnp.float32), high, mid, low], axis=1)
    used = meta.shape[1]
    meta = jnp.pad(meta, ((0, 0), (0, LANES - used))).astype(jnp.bfloat16)
    payload = jnp.concatenate([normed, meta], axis=1)

    chips = group // 2
    zigzag = []
    for chip in range(chips):
        zigzag.append((chip * 2, ((chip + 1) % chips) * 2))
        zigzag.append((chip * 2 + 1, ((chip - 1) % chips) * 2 + 1))
    swap = [(0, 1), (1, 0)]
    own = lax.all_gather(payload, "zh", axis=0, tiled=True)
    near = lax.ppermute(own, EP, zigzag)
    own_pair = lax.ppermute(own, "core", swap)
    near_pair = lax.ppermute(near, "core", swap)
    pieces = (own, own_pair, near, near_pair)
    part = own.shape[0]

    is_core = core == 1
    is_odd = odd == 1
    known = jnp.concatenate(
        [
            jnp.transpose(m)
            for m in swapped([p[:, width : width + topk] for p in pieces], is_core, is_odd)
        ],
        axis=1,
    ).astype(jnp.int32)

    experts = lax.broadcasted_iota(jnp.int32, (group, total), 0)
    hits = [(known[k : k + 1, :] == experts) for k in range(topk)]
    match = sum(h.astype(jnp.float32) for h in hits)
    before = (
        lax.broadcasted_iota(jnp.int32, (total, total), 0)
        < lax.broadcasted_iota(jnp.int32, (total, total), 1)
    ).astype(jnp.bfloat16)
    rank = jnp.dot(match.astype(jnp.bfloat16), before, preferred_element_type=jnp.float32)
    lane = jnp.stack([jnp.sum(jnp.where(h, rank, 0.0), axis=0) for h in hits]).astype(jnp.int32)
    mine = experts == me
    slot_of = jnp.sum(jnp.where(mine & (match > 0), rank + 1.0, 0.0), axis=0).astype(jnp.int32) - 1
    slot_of = jnp.concatenate(
        swapped([slot_of[k * part : (k + 1) * part] for k in range(4)], is_core, is_odd)
    )
    select = (
        lax.broadcasted_iota(jnp.int32, (most, total), 0) == slot_of[None, :]
    ).astype(jnp.bfloat16)
    rows = sum(
        jnp.dot(
            select[:, k * part : (k + 1) * part], pieces[k], preferred_element_type=jnp.float32
        )
        for k in range(4)
    )
    info = rows[:, width : width + used]
    gates = info[:, topk : 2 * topk] + info[:, 2 * topk : 3 * topk] + info[:, 3 * topk :]
    gate = jnp.sum(
        jnp.where(info[:, :topk] == me.astype(jnp.float32), gates, 0.0), axis=1, keepdims=True
    )
    rows = rows[:, :width].astype(jnp.bfloat16)

    gate_val = jnp.dot(rows, w_gate[0], preferred_element_type=jnp.float32)
    up_val = jnp.dot(rows, w_up[0], preferred_element_type=jnp.float32)
    act = (jax.nn.silu(gate_val) * up_val * gate).astype(jnp.bfloat16)
    result = lax.dot_general(
        w_down[0], act, (((0,), (1,)), ((), ())), preferred_element_type=jnp.float32
    ).astype(jnp.bfloat16)
    returned = lax.all_to_all(
        result.reshape(group, cols, most), EP, split_axis=0, concat_axis=0, tiled=True
    )
    mixed = combine(returned, known, lane)

    square = jnp.sum(mixed * mixed, axis=0)
    squares = lax.all_to_all(
        jnp.broadcast_to(square.astype(jnp.bfloat16)[None, :], (group, total)),
        EP,
        split_axis=0,
        concat_axis=0,
        tiled=True,
    )
    mean = jnp.sum(squares.astype(jnp.float32), axis=0, keepdims=True) / width
    gain = lax.dynamic_slice(final_gain, (me * cols,), (cols,))
    finished = (mixed * lax.rsqrt(mean + epsilon) * gain[:, None]).astype(jnp.bfloat16)
    finished = jnp.transpose(finished).reshape(4, part // per_dev, per_dev, cols)
    return jnp.swapaxes(finished, 0, 1).reshape(total, cols)


def solution(mesh):
    split = Mesh(mesh.devices.reshape(mesh.shape["grp"], 16, 2, 2), GRP_EP)
    return jax.shard_map(
        shards,
        mesh=split,
        in_specs=(
            P(GRP_EP, None),
            P(GRP_EP, None),
            P(GRP_EP, None),
            P(),
            P(),
            P(EP, None, None),
            P(EP, None, None),
            P(EP, None, None),
        ),
        out_specs=P("grp", EP),
        check_vma=False,
    )
```

```python
import functools

import jax
import jax.numpy as jnp
from jax import lax
from jax.experimental import pallas as pl
from jax.experimental.pallas import tpu as pltpu
from jax.sharding import Mesh
from jax.sharding import PartitionSpec as P

EP = ("zh", "zl", "core")
CHIPS = ("zh", "zl")
GRP_EP = ("grp", "zh", "zl", "core")
LANES = 128
CLASSES = 4
EPSILON = 1e-06
F32 = jnp.float32
BF16 = jnp.bfloat16

VMEM = pl.BlockSpec(memory_space=pltpu.VMEM)
SMEM = pl.BlockSpec(memory_space=pltpu.SMEM)


def by_class(parts, is_core, is_odd):
    a, b, c, d = parts
    a, b, c, d = (
        jnp.where(is_core, b, a),
        jnp.where(is_core, a, b),
        jnp.where(is_core, d, c),
        jnp.where(is_core, c, d),
    )
    return (
        jnp.where(is_odd, c, a),
        jnp.where(is_odd, d, b),
        jnp.where(is_odd, a, c),
        jnp.where(is_odd, b, d),
    )


def payload_kernel(tokens_ref, routes_ref, gates_ref, gain_ref, out_ref, meta_ref):
    width = tokens_ref.shape[1]
    per_dev = tokens_ref.shape[0]
    topk = routes_ref.shape[0]
    values = tokens_ref[...].astype(F32)
    mean = jnp.mean(values * values, axis=1, keepdims=True)
    out_ref[:, :width] = (values * lax.rsqrt(mean + EPSILON) * gain_ref[...]).astype(BF16)
    gates = gates_ref[...]
    high = gates.astype(BF16).astype(F32)
    mid = (gates - high).astype(BF16).astype(F32)
    meta_ref[...] = jnp.zeros(meta_ref.shape, F32)
    meta_ref[0:topk, 0:per_dev] = routes_ref[...].astype(F32)
    meta_ref[topk : 2 * topk, 0:per_dev] = high
    meta_ref[2 * topk : 3 * topk, 0:per_dev] = mid
    meta_ref[3 * topk : 4 * topk, 0:per_dev] = gates - high - mid
    out_ref[:, width:] = jnp.transpose(meta_ref[...])[:per_dev, :].astype(BF16)


def plan_kernel(topk, group, at_ref, a_ref, b_ref, c_ref, d_ref, rank_ref, slot_ref, gate_ref, load_ref):
    is_core = at_ref[1] == 1
    is_odd = at_ref[2] == 1
    part = a_ref.shape[0]
    meta = by_class(
        [r[...].astype(F32) for r in (a_ref, b_ref, c_ref, d_ref)], is_core, is_odd
    )
    meta = jnp.concatenate([jnp.transpose(m) for m in meta], axis=1)
    total = meta.shape[1]
    gates = meta[topk : 2 * topk] + meta[2 * topk : 3 * topk] + meta[3 * topk : 4 * topk]
    me = at_ref[0].astype(F32)
    expert = lax.broadcasted_iota(jnp.int32, (group, total), 0).astype(F32)
    match = jnp.zeros((group, total), F32)
    gate = jnp.zeros((1, total), F32)
    for k in range(topk):
        row = meta[k : k + 1, :]
        match = match + jnp.where(row == expert, 1.0, 0.0)
        gate = gate + jnp.where(row == me, gates[k : k + 1, :], 0.0)
    before = jnp.where(
        lax.broadcasted_iota(jnp.int32, (total, total), 0)
        < lax.broadcasted_iota(jnp.int32, (total, total), 1),
        1.0,
        0.0,
    ).astype(BF16)
    rank = jnp.dot(match.astype(BF16), before, preferred_element_type=F32)
    rank = jnp.where(match > 0.0, rank, -1.0)
    rank_ref[...] = rank.astype(jnp.int32)
    mine = jnp.max(jnp.where(expert == me, rank, -1.0), axis=0, keepdims=True)
    cut = lambda row: jnp.concatenate(
        by_class([row[:, k * part : (k + 1) * part] for k in range(CLASSES)], is_core, is_odd), axis=1
    )
    slot_ref[...] = cut(mine).astype(jnp.int32)
    gate_ref[...] = cut(gate)
    load = jnp.sum(match, axis=1, keepdims=True)
    pair = load + jnp.where(
        lax.broadcasted_iota(jnp.int32, (group, 1), 0) % 2 == 0,
        pltpu.roll(jnp.broadcast_to(load, (group, LANES)), group - 1, 0)[:, :1],
        0.0,
    )
    load_ref[0] = jnp.max(pair).astype(jnp.int32)


def experts_kernel(
    capacity, width, at_ref, slot_ref, gate_ref, a_ref, b_ref, c_ref, d_ref, wg_ref, wu_ref, wd_ref, keep_ref, send_ref
):
    is_core = at_ref[1] == 1
    part = a_ref.shape[0]
    total = slot_ref.shape[1]
    chips, packed, _ = keep_ref.shape
    cols = width // (2 * chips)
    slot = slot_ref[...]
    slot = jnp.where(slot < 0, -1, jnp.where(is_core, capacity - 1 - slot, slot))
    hit = lax.broadcasted_iota(jnp.int32, (capacity, total), 0) == slot
    pick = jnp.where(hit, 1.0, 0.0).astype(BF16)
    gate = jnp.sum(jnp.where(hit, gate_ref[...], 0.0), axis=1, keepdims=True)
    rows = jnp.zeros((capacity, width), F32)
    for k, ref in enumerate((a_ref, b_ref, c_ref, d_ref)):
        rows = rows + jnp.dot(
            pick[:, k * part : (k + 1) * part], ref[:, :width], preferred_element_type=F32
        )
    rows = rows.astype(BF16)
    gate_val = jnp.dot(rows, wg_ref[0], preferred_element_type=F32)
    up_val = jnp.dot(rows, wu_ref[0], preferred_element_type=F32)
    act = (gate_val * jax.nn.sigmoid(gate_val) * up_val * gate).astype(BF16)
    result = jnp.dot(act, wd_ref[0], preferred_element_type=F32)
    head = jnp.transpose(result[:LANES]).reshape(chips, 2, cols, LANES)
    even, odd = head[:, 0], head[:, 1]
    keep_ref[:, :cols, :] = jnp.where(is_core, odd, even).astype(BF16)
    send_ref[:, :cols, :] = jnp.where(is_core, even, odd).astype(BF16)
    extra = capacity - LANES
    tail = result[LANES:]
    if extra < LANES:
        tail = jnp.concatenate([tail, jnp.zeros((LANES - extra, width), F32)], axis=0)
    tail = jnp.transpose(tail).reshape(chips, 2, cols, LANES)
    even, odd = tail[:, 0], tail[:, 1]
    groups = LANES // extra
    each = cols // groups
    for ref, block in (
        (keep_ref, jnp.where(is_core, odd, even)),
        (send_ref, jnp.where(is_core, even, odd)),
    ):
        out = block[:, :each].reshape(chips * each, LANES)
        for g in range(1, groups):
            out = out + pltpu.roll(
                block[:, g * each : (g + 1) * each].reshape(chips * each, LANES), g * extra, 1
            )
        ref[:, cols:, :] = out.reshape(chips, each, LANES).astype(BF16)


def combine_kernel(capacity, rows_ref, rank_ref, out_ref, square_ref):
    cols, total = out_ref.shape
    chips = rows_ref.shape[0]
    extra = capacity - LANES
    groups = LANES // extra
    each = cols // groups
    row = lax.broadcasted_iota(jnp.int32, (2 * LANES, total), 0)
    slot = jnp.where(row < LANES, row, LANES + (row - LANES) % extra)
    col = lax.broadcasted_iota(jnp.int32, (cols, LANES), 0)
    lane = lax.broadcasted_iota(jnp.int32, (cols, LANES), 1)
    own = (col // each) == (lane // extra)

    def step(s, acc):
        low = rank_ref[pl.ds(2 * s, 1), :]
        high = rank_ref[pl.ds(2 * s + 1, 1), :]
        high = jnp.where(high < 0, -1, capacity - 1 - high)
        pick = jnp.where((slot == low) | (slot == high), 1.0, 0.0).astype(BF16)
        block = rows_ref[s].astype(F32)
        tail = jnp.concatenate([block[cols:]] * groups, axis=0)
        tail = jnp.where(own, tail, 0.0)
        left = jnp.concatenate([block[:cols], tail], axis=1).astype(BF16)
        return acc + jnp.dot(left, pick, preferred_element_type=F32)

    out = lax.fori_loop(0, chips, step, jnp.zeros((cols, total), F32), unroll=4)
    out_ref[...] = out
    square_ref[...] = jnp.sum(out * out, axis=0, keepdims=True)


def finish_kernel(width, order, squares_ref, mixed_ref, gain_ref, out_ref):
    per_dev, outer, classes = order
    total = mixed_ref.shape[1]
    sums = jnp.sum(squares_ref[...].astype(F32), axis=0)
    lines = sums.shape[0]
    mean = jnp.concatenate([sums[i : i + 1] for i in range(lines)], axis=1) / width
    scaled = mixed_ref[...] * lax.rsqrt(mean + EPSILON)
    rows = jnp.transpose(scaled) * gain_ref[...]
    rows = rows.reshape(classes, outer, per_dev, rows.shape[1])
    for k in range(classes):
        out_ref[:, k] = rows[k].astype(BF16)


def shards(tokens, routes, gate_weights, norm_gain, final_gain, w_gate, w_up, w_down):
    per_dev, width = tokens.shape
    topk = routes.shape[1]
    group = lax.axis_size(EP)
    chips = group // 2
    cols = width // group
    total = per_dev * group
    most = 2 * group
    me = lax.axis_index(EP)
    core = lax.axis_index("core")
    odd = lax.axis_index("zl")
    at = jnp.stack([me, core, odd]).astype(jnp.int32)

    payload = pl.pallas_call(
        payload_kernel,
        out_shape=jax.ShapeDtypeStruct((per_dev, width + LANES), BF16),
        scratch_shapes=[pltpu.VMEM((LANES, LANES), F32)],
    )(tokens, jnp.transpose(routes), jnp.transpose(gate_weights), norm_gain[None, :])

    zigzag = []
    for chip in range(chips):
        zigzag.append((chip * 2, ((chip + 1) % chips) * 2))
        zigzag.append((chip * 2 + 1, ((chip - 1) % chips) * 2 + 1))
    swap = [(0, 1), (1, 0)]
    own = lax.all_gather(payload, "zh", axis=0, tiled=True)
    near = lax.ppermute(own, EP, zigzag)
    own_pair = lax.ppermute(own, "core", swap)
    near_pair = lax.ppermute(near, "core", swap)
    pieces = (own, own_pair, near, near_pair)
    part = own.shape[0]

    meta_block = pl.BlockSpec((part, LANES), lambda i: (0, width // LANES))
    rank, slot, gate, load = pl.pallas_call(
        functools.partial(plan_kernel, topk, group),
        grid=(1,),
        in_specs=[SMEM] + [meta_block] * CLASSES,
        out_specs=[VMEM, VMEM, VMEM, SMEM],
        out_shape=[
            jax.ShapeDtypeStruct((group, total), jnp.int32),
            jax.ShapeDtypeStruct((1, total), jnp.int32),
            jax.ShapeDtypeStruct((1, total), F32),
            jax.ShapeDtypeStruct((1,), jnp.int32),
        ],
    )(at, *pieces)

    def branch(capacity):
        packed = cols * capacity // LANES
        message = jax.ShapeDtypeStruct((chips, packed, LANES), BF16)

        def run(at, slot, gate, rank, own, own_pair, near, near_pair, w_gate, w_up, w_down):
            keep, send = pl.pallas_call(
                functools.partial(experts_kernel, capacity, width),
                in_specs=[SMEM] + [VMEM] * 9,
                out_shape=[message, message],
            )(at, slot, gate, own, own_pair, near, near_pair, w_gate, w_up, w_down)
            both = keep + lax.ppermute(send, "core", swap)
            returned = lax.all_to_all(both, CHIPS, split_axis=0, concat_axis=0, tiled=True)
            return pl.pallas_call(
                functools.partial(combine_kernel, capacity),
                out_shape=[
                    jax.ShapeDtypeStruct((cols, total), F32),
                    jax.ShapeDtypeStruct((1, total), F32),
                ],
            )(returned, rank)

        return run

    sizes = (most * 5 // 4, most * 3 // 2, most * 2)
    level = sum((load[0] > size).astype(jnp.int32) for size in sizes[:-1])
    mixed, square = lax.switch(
        level,
        [branch(size) for size in sizes],
        at, slot, gate, rank, own, own_pair, near, near_pair, w_gate, w_up, w_down,
    )

    square = square + lax.ppermute(square, "core", swap)
    lines = total // LANES
    square = square.astype(BF16).reshape(1, lines, LANES)
    squares = lax.all_to_all(
        jnp.broadcast_to(square, (chips, lines, LANES)), CHIPS, split_axis=0, concat_axis=0, tiled=True
    )
    gain = lax.dynamic_slice(final_gain, (me * cols,), (cols,))[None, :]
    outer = part // per_dev
    finished = pl.pallas_call(
        functools.partial(finish_kernel, width, (per_dev, outer, CLASSES)),
        out_shape=jax.ShapeDtypeStruct((outer, CLASSES, per_dev, cols), BF16),
    )(squares, mixed, gain)
    return finished.reshape(total, cols)


def solution(mesh):
    split = Mesh(mesh.devices.reshape(mesh.shape["grp"], 16, 2, 2), GRP_EP)
    return jax.shard_map(
        shards,
        mesh=split,
        in_specs=(
            P(GRP_EP, None),
            P(GRP_EP, None),
            P(GRP_EP, None),
            P(),
            P(),
            P(EP, None, None),
            P(EP, None, None),
            P(EP, None, None),
        ),
        out_specs=P("grp", EP),
        check_vma=False,
    )
```

```python
import functools

import jax
import jax.numpy as jnp
from jax import lax
from jax.experimental import pallas as pl
from jax.experimental.pallas import tpu as pltpu
from jax.sharding import Mesh
from jax.sharding import PartitionSpec as P

EP = ("zh", "zl", "core")
CHIPS = ("zh", "zl")
GRP_EP = ("grp", "zh", "zl", "core")
LANES = 128
CLASSES = 4
EPSILON = 1e-06
F32 = jnp.float32
BF16 = jnp.bfloat16

VMEM = pl.BlockSpec(memory_space=pltpu.VMEM)
SMEM = pl.BlockSpec(memory_space=pltpu.SMEM)
HBM = pl.BlockSpec(memory_space=pltpu.HBM)


def by_class(parts, is_core, is_odd):
    a, b, c, d = parts
    a, b, c, d = (
        jnp.where(is_core, b, a),
        jnp.where(is_core, a, b),
        jnp.where(is_core, d, c),
        jnp.where(is_core, c, d),
    )
    return (
        jnp.where(is_odd, c, a),
        jnp.where(is_odd, d, b),
        jnp.where(is_odd, a, c),
        jnp.where(is_odd, b, d),
    )


def payload_kernel(tokens_ref, routes_ref, gates_ref, gain_ref, out_ref, meta_ref):
    width = tokens_ref.shape[1]
    per_dev = tokens_ref.shape[0]
    topk = routes_ref.shape[0]
    values = tokens_ref[...].astype(F32)
    mean = jnp.mean(values * values, axis=1, keepdims=True)
    out_ref[:, :width] = (values * lax.rsqrt(mean + EPSILON) * gain_ref[...]).astype(BF16)
    gates = gates_ref[...]
    high = gates.astype(BF16).astype(F32)
    mid = (gates - high).astype(BF16).astype(F32)
    meta_ref[...] = jnp.zeros(meta_ref.shape, F32)
    meta_ref[0:topk, 0:per_dev] = routes_ref[...].astype(F32)
    meta_ref[topk : 2 * topk, 0:per_dev] = high
    meta_ref[2 * topk : 3 * topk, 0:per_dev] = mid
    meta_ref[3 * topk : 4 * topk, 0:per_dev] = gates - high - mid
    out_ref[:, width:] = jnp.transpose(meta_ref[...])[:per_dev, :].astype(BF16)


def experts_kernel(
    topk, at_ref, a_ref, b_ref, c_ref, d_ref, wg_hbm, wu_hbm, wd_hbm,
    rank_ref, keep_ref, send_ref, load_ref, wg_ref, wu_ref, wd_ref, sems,
):
    copies = [
        pltpu.make_async_copy(src.at[0], dst, sems.at[i])
        for i, (src, dst) in enumerate(((wg_hbm, wg_ref), (wu_hbm, wu_ref), (wd_hbm, wd_ref)))
    ]
    for copy in copies:
        copy.start()
    width = wg_ref.shape[0]
    is_core = at_ref[1] == 1
    is_odd = at_ref[2] == 1
    me = at_ref[0].astype(F32)
    group, total = rank_ref.shape
    chips, cols, slots = keep_ref.shape
    per_dev = total // group
    part = a_ref.shape[0]
    outer = part // per_dev
    refs = (a_ref, b_ref, c_ref, d_ref)
    meta = by_class([r[:, width:].astype(F32) for r in refs], is_core, is_odd)
    grouped = jnp.concatenate([jnp.transpose(m) for m in meta], axis=1)
    rows = jnp.concatenate(
        [m[i * per_dev : (i + 1) * per_dev] for i in range(outer) for m in meta], axis=0
    )
    ordered = jnp.concatenate(
        [jnp.transpose(rows[i * LANES : (i + 1) * LANES]) for i in range(total // LANES)], axis=1
    )
    expert = lax.broadcasted_iota(jnp.int32, (group, total), 0).astype(F32)
    match = jnp.zeros((group, total), F32)
    for k in range(topk):
        match = match + jnp.where(ordered[k : k + 1, :] == expert, 1.0, 0.0)
    index = lax.broadcasted_iota(jnp.int32, (total, total), 0)
    at = lax.broadcasted_iota(jnp.int32, (total, total), 1)
    place = at % part // per_dev * (per_dev * CLASSES) + at // part * per_dev + at % per_dev
    counts = match.astype(BF16)
    rank = jnp.dot(
        counts, jnp.where(index < at, 1.0, 0.0).astype(BF16), preferred_element_type=F32
    )
    rank_ref[...] = jnp.where(match > 0.0, rank, -1.0)
    moved = jnp.dot(
        counts, jnp.where(index < place, 1.0, 0.0).astype(BF16), preferred_element_type=F32
    )
    slot = jnp.sum(jnp.where(expert == me, moved, 0.0), axis=0, keepdims=True)
    slot = jnp.where(is_core, slots - 1 - slot, slot)
    gates = grouped[topk : 2 * topk] + grouped[2 * topk : 3 * topk] + grouped[3 * topk : 4 * topk]
    mine = jnp.zeros((1, total), F32)
    gate = jnp.zeros((1, total), F32)
    for k in range(topk):
        named = grouped[k : k + 1, :] == me
        mine = jnp.where(named, 1.0, mine)
        gate = jnp.where(named, gates[k : k + 1, :], gate)
    slot = jnp.where(mine > 0.0, slot, -1.0).astype(jnp.int32)
    gate = jnp.concatenate(
        by_class([gate[:, k * part : (k + 1) * part] for k in range(CLASSES)], is_core, is_odd), axis=1
    )
    slot = jnp.concatenate(
        by_class([slot[:, k * part : (k + 1) * part] for k in range(CLASSES)], is_core, is_odd), axis=1
    )
    load = jnp.sum(match, axis=1, keepdims=True)
    pair = load + jnp.where(
        lax.broadcasted_iota(jnp.int32, (group, 1), 0) % 2 == 0,
        pltpu.roll(jnp.broadcast_to(load, (group, LANES)), group - 1, 0)[:, :1],
        0.0,
    )
    load_ref[0] = jnp.max(pair).astype(jnp.int32)

    hit = lax.broadcasted_iota(jnp.int32, (slots, total), 0) == slot
    pick = jnp.where(hit, 1.0, 0.0).astype(BF16)
    gate = jnp.sum(jnp.where(hit, gate, 0.0), axis=1, keepdims=True)
    picked = jnp.zeros((slots, width), F32)
    for k, ref in enumerate(refs):
        picked = picked + jnp.dot(
            pick[:, k * part : (k + 1) * part], ref[:, :width], preferred_element_type=F32
        )
    picked = picked.astype(BF16)
    copies[0].wait()
    gate_val = jnp.dot(picked, wg_ref[...], preferred_element_type=F32)
    copies[1].wait()
    up_val = jnp.dot(picked, wu_ref[...], preferred_element_type=F32)
    act = (gate_val * jax.nn.sigmoid(gate_val) * up_val * gate).astype(BF16)
    copies[2].wait()
    result = jnp.dot(act, wd_ref[...], preferred_element_type=F32)
    result = jnp.transpose(result).reshape(chips, 2, cols, slots)
    even, odd = result[:, 0], result[:, 1]
    keep_ref[...] = jnp.where(is_core, odd, even).astype(BF16)
    send_ref[...] = jnp.where(is_core, even, odd).astype(BF16)


def pack_kernel(capacity, at_ref, keep_ref, got_ref, out_ref):
    is_core = at_ref[1] == 1
    chips, cols, slots = keep_ref.shape
    extra = capacity - slots
    groups = slots // extra
    each = cols // groups
    keep = keep_ref[...].astype(F32).reshape(chips * cols, slots)
    got = got_ref[...].astype(F32).reshape(chips * cols, slots)
    low = jnp.where(is_core, got, keep)
    high = jnp.where(is_core, keep, got)
    if groups == 1:
        main, tail = low, high
    else:
        high = pltpu.roll(high, extra, 1)
        spill = lax.broadcasted_iota(jnp.int32, high.shape, 1) < extra
        main = low + jnp.where(spill, 0.0, high)
        tail = jnp.where(spill, high, 0.0)
    out_ref[:, :cols, :] = main.reshape(chips, cols, slots).astype(BF16)
    tail = tail.reshape(chips, cols, slots)
    out = tail[:, :each].reshape(chips * each, slots)
    for g in range(1, groups):
        out = out + pltpu.roll(
            tail[:, g * each : (g + 1) * each].reshape(chips * each, slots), g * extra, 1
        )
    out_ref[:, cols:, :] = out.reshape(chips, each, slots).astype(BF16)


def combine_kernel(capacity, rows_ref, rank_ref, out_ref, square_ref):
    cols, total = out_ref.shape
    chips = rows_ref.shape[0]
    extra = capacity - LANES
    groups = LANES // extra
    each = cols // groups
    row = lax.broadcasted_iota(jnp.int32, (2 * LANES, total), 0)
    slot = jnp.where(row < LANES, row, LANES + (row - LANES) % extra).astype(F32).astype(BF16)
    col = lax.broadcasted_iota(jnp.int32, (cols, LANES), 0)
    lane = lax.broadcasted_iota(jnp.int32, (cols, LANES), 1)
    own = (col // each) == (lane // extra)
    one = jnp.ones((), BF16)
    zero = jnp.zeros((), BF16)

    def step(s, acc):
        low = rank_ref[pl.ds(2 * s, 1), :]
        high = rank_ref[pl.ds(2 * s + 1, 1), :]
        high = jnp.where(high < 0.0, -1.0, capacity - 1.0 - high)
        pick = jnp.where((slot == low.astype(BF16)) | (slot == high.astype(BF16)), one, zero)
        block = rows_ref[s].astype(F32)
        tail = jnp.concatenate([block[cols:]] * groups, axis=0)
        tail = jnp.where(own, tail, 0.0)
        left = jnp.concatenate([block[:cols], tail], axis=1).astype(BF16)
        return acc + jnp.dot(left, pick, preferred_element_type=F32)

    out = lax.fori_loop(0, chips, step, jnp.zeros((cols, total), F32), unroll=4)
    out_ref[...] = out
    square = jnp.sum(out * out, axis=0, keepdims=True)
    for i in range(total // LANES):
        square_ref[:, i : i + 1, :] = jnp.broadcast_to(
            square[None, :, i * LANES : (i + 1) * LANES], (chips, 1, LANES)
        ).astype(BF16)


def finish_kernel(width, mine_ref, other_ref, mixed_ref, gain_ref, out_ref):
    sums = jnp.sum(mine_ref[...].astype(F32), axis=0) + jnp.sum(other_ref[...].astype(F32), axis=0)
    mean = jnp.concatenate([sums[i : i + 1] for i in range(sums.shape[0])], axis=1) / width
    out_ref[...] = (mixed_ref[...] * lax.rsqrt(mean + EPSILON) * gain_ref[...]).astype(BF16)


def shards(tokens, routes, gate_weights, norm_gain, final_gain, w_gate, w_up, w_down):
    per_dev, width = tokens.shape
    topk = routes.shape[1]
    group = lax.axis_size(EP)
    chips = group // 2
    cols = width // group
    total = per_dev * group
    most = 2 * group
    me = lax.axis_index(EP)
    core = lax.axis_index("core")
    odd = lax.axis_index("zl")
    at = jnp.stack([me, core, odd]).astype(jnp.int32)

    payload = pl.pallas_call(
        payload_kernel,
        out_shape=jax.ShapeDtypeStruct((per_dev, width + LANES), BF16),
        scratch_shapes=[pltpu.VMEM((LANES, LANES), F32)],
    )(tokens, jnp.transpose(routes), jnp.transpose(gate_weights), norm_gain[None, :])

    zigzag = []
    for chip in range(chips):
        zigzag.append((chip * 2, ((chip + 1) % chips) * 2))
        zigzag.append((chip * 2 + 1, ((chip - 1) % chips) * 2 + 1))
    swap = [(0, 1), (1, 0)]
    own = lax.all_gather(payload, "zh", axis=0, tiled=True)
    near = lax.ppermute(own, EP, zigzag)
    own_pair = lax.ppermute(own, "core", swap)
    near_pair = lax.ppermute(near, "core", swap)
    pieces = (own, own_pair, near, near_pair)
    part = own.shape[0]

    window = jax.ShapeDtypeStruct((chips, cols, LANES), BF16)
    rank, keep, send, load = pl.pallas_call(
        functools.partial(experts_kernel, topk),
        in_specs=[SMEM] + [VMEM] * CLASSES + [HBM] * 3,
        out_specs=[VMEM, VMEM, VMEM, SMEM],
        out_shape=[
            jax.ShapeDtypeStruct((group, total), F32),
            window,
            window,
            jax.ShapeDtypeStruct((1,), jnp.int32),
        ],
        scratch_shapes=[
            pltpu.VMEM(w_gate.shape[1:], BF16),
            pltpu.VMEM(w_up.shape[1:], BF16),
            pltpu.VMEM(w_down.shape[1:], BF16),
            pltpu.SemaphoreType.DMA((3,)),
        ],
        compiler_params=pltpu.CompilerParams(vmem_limit_bytes=40 << 20),
    )(at, *pieces, w_gate, w_up, w_down)
    got = lax.ppermute(send, "core", swap)
    lines = total // LANES

    def branch(capacity):
        packed = cols * capacity // LANES

        def run(at, keep, got, rank):
            both = pl.pallas_call(
                functools.partial(pack_kernel, capacity),
                in_specs=[SMEM, VMEM, VMEM],
                out_shape=jax.ShapeDtypeStruct((chips, packed, LANES), BF16),
                compiler_params=pltpu.CompilerParams(vmem_limit_bytes=16 << 20),
            )(at, keep, got)
            returned = lax.all_to_all(both, CHIPS, split_axis=0, concat_axis=0, tiled=True)
            return pl.pallas_call(
                functools.partial(combine_kernel, capacity),
                out_shape=[
                    jax.ShapeDtypeStruct((cols, total), F32),
                    jax.ShapeDtypeStruct((chips, lines, LANES), BF16),
                ],
                compiler_params=pltpu.CompilerParams(vmem_limit_bytes=16 << 20),
            )(returned, rank)

        return run

    sizes = (most * 5 // 4, most * 3 // 2, most * 2)
    level = sum((load[0] > size).astype(jnp.int32) for size in sizes[:-1])
    mixed, square = lax.switch(level, [branch(size) for size in sizes], at, keep, got, rank)

    squares = lax.all_to_all(square, CHIPS, split_axis=0, concat_axis=0, tiled=True)
    gain = lax.dynamic_slice(final_gain, (me * cols,), (cols,))[:, None]
    finished = pl.pallas_call(
        functools.partial(finish_kernel, width),
        out_shape=jax.ShapeDtypeStruct((cols, total), BF16),
    )(squares, lax.ppermute(squares, "core", swap), mixed, gain)
    return jnp.transpose(finished)


def solution(mesh):
    split = Mesh(mesh.devices.reshape(mesh.shape["grp"], 16, 2, 2), GRP_EP)
    return jax.shard_map(
        shards,
        mesh=split,
        in_specs=(
            P(GRP_EP, None),
            P(GRP_EP, None),
            P(GRP_EP, None),
            P(),
            P(),
            P(EP, None, None),
            P(EP, None, None),
            P(EP, None, None),
        ),
        out_specs=P("grp", EP),
        check_vma=False,
    )
```

```python
import functools

import jax
import jax.numpy as jnp
from jax import lax
from jax.experimental import pallas as pl
from jax.experimental.pallas import tpu as pltpu
from jax.sharding import Mesh
from jax.sharding import PartitionSpec as P

EP = ("zh", "zl", "core")
CHIPS = ("zh", "zl")
GRP_EP = ("grp", "zh", "zl", "core")
LANES = 128
CLASSES = 4
EPSILON = 1e-06
F32 = jnp.float32
BF16 = jnp.bfloat16

VMEM = pl.BlockSpec(memory_space=pltpu.VMEM)
SMEM = pl.BlockSpec(memory_space=pltpu.SMEM)
HBM = pl.BlockSpec(memory_space=pltpu.HBM)


def by_class(parts, is_core, is_odd):
    a, b, c, d = parts
    a, b, c, d = (
        jnp.where(is_core, b, a),
        jnp.where(is_core, a, b),
        jnp.where(is_core, d, c),
        jnp.where(is_core, c, d),
    )
    return (
        jnp.where(is_odd, c, a),
        jnp.where(is_odd, d, b),
        jnp.where(is_odd, a, c),
        jnp.where(is_odd, b, d),
    )


def payload_kernel(tokens_ref, routes_ref, gates_ref, gain_ref, out_ref, meta_ref):
    width = tokens_ref.shape[1]
    per_dev = tokens_ref.shape[0]
    topk = routes_ref.shape[0]
    values = tokens_ref[...].astype(F32)
    mean = jnp.mean(values * values, axis=1, keepdims=True)
    out_ref[:, :width] = (values * lax.rsqrt(mean + EPSILON) * gain_ref[...]).astype(BF16)
    gates = gates_ref[...]
    high = gates.astype(BF16).astype(F32)
    mid = (gates - high).astype(BF16).astype(F32)
    meta_ref[...] = jnp.zeros(meta_ref.shape, F32)
    meta_ref[0:topk, 0:per_dev] = routes_ref[...].astype(F32)
    meta_ref[topk : 2 * topk, 0:per_dev] = high
    meta_ref[2 * topk : 3 * topk, 0:per_dev] = mid
    meta_ref[3 * topk : 4 * topk, 0:per_dev] = gates - high - mid
    out_ref[:, width:] = jnp.transpose(meta_ref[...])[:per_dev, :].astype(BF16)


def experts_kernel(
    topk, at_ref, a_ref, b_ref, c_ref, d_ref, wg_hbm, wu_hbm, wd_hbm,
    rank_ref, keep_ref, send_ref, load_ref, wg_ref, wu_ref, wd_ref, sems,
):
    copies = [
        pltpu.make_async_copy(src.at[0], dst, sems.at[i])
        for i, (src, dst) in enumerate(((wg_hbm, wg_ref), (wu_hbm, wu_ref), (wd_hbm, wd_ref)))
    ]
    for copy in copies:
        copy.start()
    width = wg_ref.shape[0]
    is_core = at_ref[1] == 1
    is_odd = at_ref[2] == 1
    me = at_ref[0].astype(F32)
    group, total = rank_ref.shape
    chips, cols, slots = keep_ref.shape
    per_dev = total // group
    part = a_ref.shape[0]
    outer = part // per_dev
    refs = (a_ref, b_ref, c_ref, d_ref)
    meta = by_class([r[:, width:].astype(F32) for r in refs], is_core, is_odd)
    grouped = jnp.concatenate([jnp.transpose(m) for m in meta], axis=1)
    rows = jnp.concatenate(
        [m[i * per_dev : (i + 1) * per_dev] for i in range(outer) for m in meta], axis=0
    )
    ordered = jnp.concatenate(
        [jnp.transpose(rows[i * LANES : (i + 1) * LANES]) for i in range(total // LANES)], axis=1
    )
    expert = lax.broadcasted_iota(jnp.int32, (group, total), 0).astype(F32)
    match = jnp.zeros((group, total), F32)
    for k in range(topk):
        match = match + jnp.where(ordered[k : k + 1, :] == expert, 1.0, 0.0)
    index = lax.broadcasted_iota(jnp.int32, (total, total), 0)
    at = lax.broadcasted_iota(jnp.int32, (total, total), 1)
    place = at % part // per_dev * (per_dev * CLASSES) + at // part * per_dev + at % per_dev
    counts = match.astype(BF16)
    rank = jnp.dot(
        counts, jnp.where(index < at, 1.0, 0.0).astype(BF16), preferred_element_type=F32
    )
    rank_ref[...] = jnp.where(match > 0.0, rank, -1.0)
    moved = jnp.dot(
        counts, jnp.where(index < place, 1.0, 0.0).astype(BF16), preferred_element_type=F32
    )
    slot = jnp.sum(jnp.where(expert == me, moved, 0.0), axis=0, keepdims=True)
    slot = jnp.where(is_core, slots - 1 - slot, slot)
    gates = grouped[topk : 2 * topk] + grouped[2 * topk : 3 * topk] + grouped[3 * topk : 4 * topk]
    mine = jnp.zeros((1, total), F32)
    gate = jnp.zeros((1, total), F32)
    for k in range(topk):
        named = grouped[k : k + 1, :] == me
        mine = jnp.where(named, 1.0, mine)
        gate = jnp.where(named, gates[k : k + 1, :], gate)
    slot = jnp.where(mine > 0.0, slot, -1.0).astype(jnp.int32)
    gate = jnp.concatenate(
        by_class([gate[:, k * part : (k + 1) * part] for k in range(CLASSES)], is_core, is_odd), axis=1
    )
    slot = jnp.concatenate(
        by_class([slot[:, k * part : (k + 1) * part] for k in range(CLASSES)], is_core, is_odd), axis=1
    )
    load = jnp.sum(match, axis=1, keepdims=True)
    pair = load + jnp.where(
        lax.broadcasted_iota(jnp.int32, (group, 1), 0) % 2 == 0,
        pltpu.roll(jnp.broadcast_to(load, (group, LANES)), group - 1, 0)[:, :1],
        0.0,
    )
    load_ref[0] = jnp.max(pair).astype(jnp.int32)

    hit = lax.broadcasted_iota(jnp.int32, (slots, total), 0) == slot
    pick = jnp.where(hit, 1.0, 0.0).astype(BF16)
    gate = jnp.sum(jnp.where(hit, gate, 0.0), axis=1, keepdims=True)
    picked = jnp.zeros((slots, width), F32)
    for k, ref in enumerate(refs):
        picked = picked + jnp.dot(
            pick[:, k * part : (k + 1) * part], ref[:, :width], preferred_element_type=F32
        )
    picked = picked.astype(BF16)
    copies[0].wait()
    gate_val = jnp.dot(picked, wg_ref[...], preferred_element_type=F32)
    copies[1].wait()
    up_val = jnp.dot(picked, wu_ref[...], preferred_element_type=F32)
    act = (gate_val * jax.nn.sigmoid(gate_val) * up_val * gate).astype(BF16)
    copies[2].wait()
    result = jnp.dot(act, wd_ref[...], preferred_element_type=F32)
    result = jnp.transpose(result).reshape(chips, 2, cols, slots)
    even, odd = result[:, 0], result[:, 1]
    keep_ref[...] = jnp.where(is_core, odd, even).astype(BF16)
    send_ref[...] = jnp.where(is_core, even, odd).astype(BF16)


def pack_kernel(capacity, at_ref, keep_ref, got_ref, out_ref):
    is_core = at_ref[1] == 1
    chips, cols, slots = keep_ref.shape
    extra = capacity - slots
    groups = slots // extra
    each = cols // groups
    keep = keep_ref[...].astype(F32).reshape(chips * cols, slots)
    got = got_ref[...].astype(F32).reshape(chips * cols, slots)
    low = jnp.where(is_core, got, keep)
    high = jnp.where(is_core, keep, got)
    if groups == 1:
        main, tail = low, high
    else:
        high = pltpu.roll(high, extra, 1)
        spill = lax.broadcasted_iota(jnp.int32, high.shape, 1) < extra
        main = low + jnp.where(spill, 0.0, high)
        tail = jnp.where(spill, high, 0.0)
    out_ref[:, :cols, :] = main.reshape(chips, cols, slots).astype(BF16)
    tail = tail.reshape(chips, cols, slots)
    out = tail[:, :each].reshape(chips * each, slots)
    for g in range(1, groups):
        out = out + pltpu.roll(
            tail[:, g * each : (g + 1) * each].reshape(chips * each, slots), g * extra, 1
        )
    out_ref[:, cols:, :] = out.reshape(chips, each, slots).astype(BF16)


def combine_kernel(capacity, rows_ref, rank_ref, out_ref, square_ref):
    cols, total = out_ref.shape
    chips = rows_ref.shape[0]
    extra = capacity - LANES
    groups = LANES // extra
    each = cols // groups
    row = lax.broadcasted_iota(jnp.int32, (2 * LANES, total), 0)
    slot = jnp.where(row < LANES, row, LANES + (row - LANES) % extra).astype(F32).astype(BF16)
    col = lax.broadcasted_iota(jnp.int32, (cols, LANES), 0)
    lane = lax.broadcasted_iota(jnp.int32, (cols, LANES), 1)
    own = (col // each) == (lane // extra)
    one = jnp.ones((), BF16)
    zero = jnp.zeros((), BF16)

    def step(s, acc):
        low = rank_ref[pl.ds(2 * s, 1), :]
        high = rank_ref[pl.ds(2 * s + 1, 1), :]
        high = jnp.where(high < 0.0, -1.0, capacity - 1.0 - high)
        pick = jnp.where((slot == low.astype(BF16)) | (slot == high.astype(BF16)), one, zero)
        block = rows_ref[s].astype(F32)
        tail = jnp.concatenate([block[cols:]] * groups, axis=0)
        tail = jnp.where(own, tail, 0.0)
        left = jnp.concatenate([block[:cols], tail], axis=1).astype(BF16)
        return acc + jnp.dot(left, pick, preferred_element_type=F32)

    out = lax.fori_loop(0, chips, step, jnp.zeros((cols, total), F32), unroll=4)
    out_ref[...] = out
    square = jnp.sum(out * out, axis=0, keepdims=True)
    for i in range(total // LANES):
        square_ref[:, i : i + 1, :] = jnp.broadcast_to(
            square[None, :, i * LANES : (i + 1) * LANES], (chips, 1, LANES)
        ).astype(BF16)


def finish_kernel(width, at_ref, mine_ref, other_ref, mixed_ref, gain_ref, out_ref):
    sums = jnp.sum(mine_ref[...].astype(F32), axis=0) + jnp.sum(other_ref[...].astype(F32), axis=0)
    mean = jnp.concatenate([sums[i : i + 1] for i in range(sums.shape[0])], axis=1) / width
    cols = mixed_ref.shape[0]
    each = LANES // cols
    me = at_ref[0]
    gain = jnp.broadcast_to(gain_ref[pl.ds(me // each, 1), :], (LANES, LANES))
    gain = pltpu.roll(gain, (each - me % each) % each * cols, 1)
    gain = jnp.transpose(gain)[:cols, :1]
    out_ref[...] = (mixed_ref[...] * lax.rsqrt(mean + EPSILON) * gain).astype(BF16)


def shards(tokens, routes, gate_weights, norm_gain, final_gain, w_gate, w_up, w_down):
    per_dev, width = tokens.shape
    topk = routes.shape[1]
    group = lax.axis_size(EP)
    chips = group // 2
    cols = width // group
    total = per_dev * group
    most = 2 * group
    me = lax.axis_index(EP)
    core = lax.axis_index("core")
    odd = lax.axis_index("zl")
    at = jnp.stack([me, core, odd]).astype(jnp.int32)

    payload = pl.pallas_call(
        payload_kernel,
        out_shape=jax.ShapeDtypeStruct((per_dev, width + LANES), BF16),
        scratch_shapes=[pltpu.VMEM((LANES, LANES), F32)],
    )(tokens, jnp.transpose(routes), jnp.transpose(gate_weights), norm_gain[None, :])

    zigzag = []
    for chip in range(chips):
        zigzag.append((chip * 2, ((chip + 1) % chips) * 2))
        zigzag.append((chip * 2 + 1, ((chip - 1) % chips) * 2 + 1))
    swap = [(0, 1), (1, 0)]
    own = lax.all_gather(payload, "zh", axis=0, tiled=True)
    near = lax.ppermute(own, EP, zigzag)
    own_pair = lax.ppermute(own, "core", swap)
    near_pair = lax.ppermute(near, "core", swap)
    pieces = (own, own_pair, near, near_pair)
    part = own.shape[0]

    window = jax.ShapeDtypeStruct((chips, cols, LANES), BF16)
    rank, keep, send, load = pl.pallas_call(
        functools.partial(experts_kernel, topk),
        in_specs=[SMEM] + [VMEM] * CLASSES + [HBM] * 3,
        out_specs=[VMEM, VMEM, VMEM, SMEM],
        out_shape=[
            jax.ShapeDtypeStruct((group, total), F32),
            window,
            window,
            jax.ShapeDtypeStruct((1,), jnp.int32),
        ],
        scratch_shapes=[
            pltpu.VMEM(w_gate.shape[1:], BF16),
            pltpu.VMEM(w_up.shape[1:], BF16),
            pltpu.VMEM(w_down.shape[1:], BF16),
            pltpu.SemaphoreType.DMA((3,)),
        ],
        compiler_params=pltpu.CompilerParams(vmem_limit_bytes=50 << 20),
    )(at, *pieces, w_gate, w_up, w_down)
    got = lax.ppermute(send, "core", swap)
    lines = total // LANES

    def branch(capacity):
        packed = cols * capacity // LANES

        def run(at, keep, got, rank):
            both = pl.pallas_call(
                functools.partial(pack_kernel, capacity),
                in_specs=[SMEM, VMEM, VMEM],
                out_shape=jax.ShapeDtypeStruct((chips, packed, LANES), BF16),
                compiler_params=pltpu.CompilerParams(vmem_limit_bytes=16 << 20),
            )(at, keep, got)
            returned = lax.all_to_all(both, CHIPS, split_axis=0, concat_axis=0, tiled=True)
            return pl.pallas_call(
                functools.partial(combine_kernel, capacity),
                in_specs=[VMEM, VMEM],
                out_shape=[
                    jax.ShapeDtypeStruct((cols, total), F32),
                    jax.ShapeDtypeStruct((chips, lines, LANES), BF16),
                ],
                compiler_params=pltpu.CompilerParams(vmem_limit_bytes=16 << 20),
            )(returned, rank)

        return run

    sizes = (most * 5 // 4, most * 3 // 2, most * 2)
    level = sum((load[0] > size).astype(jnp.int32) for size in sizes[:-1])
    mixed, square = lax.switch(level, [branch(size) for size in sizes], at, keep, got, rank)

    squares = lax.all_to_all(square, CHIPS, split_axis=0, concat_axis=0, tiled=True)
    finished = pl.pallas_call(
        functools.partial(finish_kernel, width),
        in_specs=[SMEM] + [VMEM] * 4,
        out_shape=jax.ShapeDtypeStruct((cols, total), BF16),
        compiler_params=pltpu.CompilerParams(vmem_limit_bytes=16 << 20),
    )(at, squares, lax.ppermute(squares, "core", swap), mixed, final_gain.reshape(-1, LANES))
    return jnp.transpose(finished)


def solution(mesh):
    split = Mesh(mesh.devices.reshape(mesh.shape["grp"], 16, 2, 2), GRP_EP)
    return jax.shard_map(
        shards,
        mesh=split,
        in_specs=(
            P(GRP_EP, None),
            P(GRP_EP, None),
            P(GRP_EP, None),
            P(),
            P(),
            P(EP, None, None),
            P(EP, None, None),
            P(EP, None, None),
        ),
        out_specs=P("grp", EP),
        check_vma=False,
    )
```

```python
import functools

import jax
import jax.numpy as jnp
from jax import lax
from jax.experimental import pallas as pl
from jax.experimental.pallas import tpu as pltpu
from jax.sharding import Mesh
from jax.sharding import PartitionSpec as P

EP = ("zh", "zl", "core")
CHIPS = ("zh", "zl")
GRP_EP = ("grp", "zh", "zl", "core")
LANES = 128
CLASSES = 4
EPSILON = 1e-06
F32 = jnp.float32
BF16 = jnp.bfloat16

VMEM = pl.BlockSpec(memory_space=pltpu.VMEM)
SMEM = pl.BlockSpec(memory_space=pltpu.SMEM)
HBM = pl.BlockSpec(memory_space=pltpu.HBM)


def by_class(parts, is_core, is_odd):
    a, b, c, d = parts
    a, b, c, d = (
        jnp.where(is_core, b, a),
        jnp.where(is_core, a, b),
        jnp.where(is_core, d, c),
        jnp.where(is_core, c, d),
    )
    return (
        jnp.where(is_odd, c, a),
        jnp.where(is_odd, d, b),
        jnp.where(is_odd, a, c),
        jnp.where(is_odd, b, d),
    )


def payload_kernel(tokens_ref, routes_ref, gates_ref, gain_ref, out_ref, meta_ref):
    width = tokens_ref.shape[1]
    per_dev = tokens_ref.shape[0]
    topk = routes_ref.shape[0]
    values = tokens_ref[...].astype(F32)
    mean = jnp.mean(values * values, axis=1, keepdims=True)
    out_ref[:, :width] = (values * lax.rsqrt(mean + EPSILON) * gain_ref[...]).astype(BF16)
    gates = gates_ref[...]
    high = gates.astype(BF16).astype(F32)
    mid = (gates - high).astype(BF16).astype(F32)
    meta_ref[...] = jnp.zeros(meta_ref.shape, F32)
    meta_ref[0:topk, 0:per_dev] = routes_ref[...].astype(F32)
    meta_ref[topk : 2 * topk, 0:per_dev] = high
    meta_ref[2 * topk : 3 * topk, 0:per_dev] = mid
    meta_ref[3 * topk : 4 * topk, 0:per_dev] = gates - high - mid
    out_ref[:, width:] = jnp.transpose(meta_ref[...])[:per_dev, :].astype(BF16)


def shed(load, capacity):
    group = load.shape[0]
    even = lax.broadcasted_iota(jnp.int32, load.shape, 0) % 2 == 0
    at = lambda x, d: pltpu.roll(x, (-d) % group, 0)
    chip = load + jnp.where(even, at(load, 1), at(load, -1))
    half = capacity // 2
    over = jnp.where(chip > capacity, jnp.maximum(load - half, 0.0), 0.0)
    kept = load - over
    settled = jnp.where(even, kept + at(kept, 1) + at(over, -2) + at(over, 3), 0.0)
    return kept, chip, settled


def windows(at_ref, keep_ref, got_ref):
    is_core = at_ref[1] == 1
    chips, cols, slots = keep_ref.shape
    keep = keep_ref[...].astype(F32).reshape(chips * cols, slots)
    got = got_ref[...].astype(F32).reshape(chips * cols, slots)
    return jnp.where(is_core, got, keep), jnp.where(is_core, keep, got)


def spill_kernel(at_ref, keep_ref, got_ref, right_ref, left_ref):
    low, high = windows(at_ref, keep_ref, got_ref)
    rows = right_ref.shape[0]
    side = LANES // 2
    lane = lax.broadcasted_iota(jnp.int32, (rows, LANES), 1)
    right_ref[...] = jnp.where(
        lane >= side, low[:rows], pltpu.roll(low[rows:], side, 1)
    ).astype(BF16)
    left_ref[...] = jnp.where(
        lane < side, high[:rows], pltpu.roll(high[rows:], side, 1)
    ).astype(BF16)


def pooled_pack_kernel(capacity, at_ref, keep_ref, got_ref, right_ref, left_ref, load_ref, out_ref):
    low, high = windows(at_ref, keep_ref, got_ref)
    chips, cols, slots = keep_ref.shape
    extra = capacity - slots
    half = capacity // 2
    load = load_ref[...]
    group = load.shape[0]
    kept, _, _ = shed(load, capacity)
    over = load - kept
    row = lax.broadcasted_iota(jnp.int32, load.shape, 0)
    first = at_ref[0] // 2 * 2
    one = lambda x, e: jnp.max(jnp.where(row == (e + group) % group, x, 0.0)).astype(jnp.int32)
    kept_low, kept_high = one(kept, first), one(kept, first + 1)
    from_left, from_right = one(over, first - 2), one(over, first + 3)
    lane = lax.broadcasted_iota(jnp.int32, low.shape, 1)
    side = LANES // 2
    unfold = lambda ref: jnp.concatenate(
        [ref[...].astype(F32), pltpu.roll(ref[...].astype(F32), side, 1)], axis=0
    )
    low = jnp.where(lane < kept_low, low, 0.0)
    high = jnp.where(lane >= slots - kept_high, high, 0.0)
    left = unfold(right_ref)
    left = jnp.where((lane >= half) & (lane < half + from_left), left, 0.0)
    right = unfold(left_ref)
    top = slots - 1 - half
    right = jnp.where((lane <= top) & (lane > top - from_right), right, 0.0)
    high = pltpu.roll(high, extra, 1)
    left = pltpu.roll(left, (kept_low - half + slots) % slots, 1)
    right = pltpu.roll(right, (capacity - 1 - kept_high - top + slots) % slots, 1)
    main = low + jnp.where(lane >= extra, high, 0.0)
    main = main + jnp.where(lane >= kept_low, left, 0.0)
    main = main + jnp.where(lane >= extra - kept_high, right, 0.0)
    tail = jnp.where(lane < extra, high, 0.0)
    tail = tail + jnp.where(lane < kept_low, left, 0.0)
    tail = tail + jnp.where(lane < extra - kept_high, right, 0.0)
    store_packed(main, tail, extra, out_ref)


def store_packed(main, tail, extra, out_ref):
    chips, packed, slots = out_ref.shape
    cols = main.shape[0] // chips
    groups = slots // extra
    each = cols // groups
    out_ref[:, :cols, :] = main.reshape(chips, cols, slots).astype(BF16)
    tail = tail.reshape(chips, cols, slots)
    out = tail[:, :each].reshape(chips * each, slots)
    for g in range(1, groups):
        out = out + pltpu.roll(
            tail[:, g * each : (g + 1) * each].reshape(chips * each, slots), g * extra, 1
        )
    out_ref[:, cols:, :] = out.reshape(chips, each, slots).astype(BF16)


def experts_kernel(
    topk, sizes, at_ref, a_ref, b_ref, c_ref, d_ref, wg_hbm, wu_hbm, wd_hbm,
    rank_ref, keep_ref, send_ref, load_ref, level_ref, wg_ref, wu_ref, wd_ref, sems,
):
    copies = [
        pltpu.make_async_copy(src.at[0], dst, sems.at[i])
        for i, (src, dst) in enumerate(((wg_hbm, wg_ref), (wu_hbm, wu_ref), (wd_hbm, wd_ref)))
    ]
    for copy in copies:
        copy.start()
    width = wg_ref.shape[0]
    is_core = at_ref[1] == 1
    is_odd = at_ref[2] == 1
    me = at_ref[0].astype(F32)
    group, total = rank_ref.shape
    chips, cols, slots = keep_ref.shape
    per_dev = total // group
    part = a_ref.shape[0]
    outer = part // per_dev
    refs = (a_ref, b_ref, c_ref, d_ref)
    meta = by_class([r[:, width:].astype(F32) for r in refs], is_core, is_odd)
    grouped = jnp.concatenate([jnp.transpose(m) for m in meta], axis=1)
    rows = jnp.concatenate(
        [m[i * per_dev : (i + 1) * per_dev] for i in range(outer) for m in meta], axis=0
    )
    ordered = jnp.concatenate(
        [jnp.transpose(rows[i * LANES : (i + 1) * LANES]) for i in range(total // LANES)], axis=1
    )
    expert = lax.broadcasted_iota(jnp.int32, (group, total), 0).astype(F32)
    match = jnp.zeros((group, total), F32)
    for k in range(topk):
        match = match + jnp.where(ordered[k : k + 1, :] == expert, 1.0, 0.0)
    index = lax.broadcasted_iota(jnp.int32, (total, total), 0)
    at = lax.broadcasted_iota(jnp.int32, (total, total), 1)
    place = at % part // per_dev * (per_dev * CLASSES) + at // part * per_dev + at % per_dev
    counts = match.astype(BF16)
    rank = jnp.dot(
        counts, jnp.where(index < at, 1.0, 0.0).astype(BF16), preferred_element_type=F32
    )
    rank_ref[...] = jnp.where(match > 0.0, rank, -1.0)
    moved = jnp.dot(
        counts, jnp.where(index < place, 1.0, 0.0).astype(BF16), preferred_element_type=F32
    )
    slot = jnp.sum(jnp.where(expert == me, moved, 0.0), axis=0, keepdims=True)
    slot = jnp.where(is_core, slots - 1 - slot, slot)
    gates = grouped[topk : 2 * topk] + grouped[2 * topk : 3 * topk] + grouped[3 * topk : 4 * topk]
    mine = jnp.zeros((1, total), F32)
    gate = jnp.zeros((1, total), F32)
    for k in range(topk):
        named = grouped[k : k + 1, :] == me
        mine = jnp.where(named, 1.0, mine)
        gate = jnp.where(named, gates[k : k + 1, :], gate)
    slot = jnp.where(mine > 0.0, slot, -1.0).astype(jnp.int32)
    gate = jnp.concatenate(
        by_class([gate[:, k * part : (k + 1) * part] for k in range(CLASSES)], is_core, is_odd), axis=1
    )
    slot = jnp.concatenate(
        by_class([slot[:, k * part : (k + 1) * part] for k in range(CLASSES)], is_core, is_odd), axis=1
    )
    load = jnp.broadcast_to(jnp.sum(match, axis=1, keepdims=True), (group, LANES))
    load_ref[...] = load
    kept, chip, settled = shed(load, sizes[0])
    most = jnp.max(chip).astype(jnp.int32)
    fits = (jnp.max(settled).astype(jnp.int32) <= sizes[0]).astype(jnp.int32)
    level_ref[0] = jnp.where(
        most <= sizes[0], 0, jnp.where(most <= sizes[1], 1, 3 - fits)
    ).astype(jnp.int32)

    hit = lax.broadcasted_iota(jnp.int32, (slots, total), 0) == slot
    pick = jnp.where(hit, 1.0, 0.0).astype(BF16)
    gate = jnp.sum(jnp.where(hit, gate, 0.0), axis=1, keepdims=True)
    picked = jnp.zeros((slots, width), F32)
    for k, ref in enumerate(refs):
        picked = picked + jnp.dot(
            pick[:, k * part : (k + 1) * part], ref[:, :width], preferred_element_type=F32
        )
    picked = picked.astype(BF16)
    copies[0].wait()
    gate_val = jnp.dot(picked, wg_ref[...], preferred_element_type=F32)
    copies[1].wait()
    up_val = jnp.dot(picked, wu_ref[...], preferred_element_type=F32)
    act = (gate_val * jax.nn.sigmoid(gate_val) * up_val * gate).astype(BF16)
    copies[2].wait()
    result = jnp.dot(act, wd_ref[...], preferred_element_type=F32)
    result = jnp.transpose(result).reshape(chips, 2, cols, slots)
    even, odd = result[:, 0], result[:, 1]
    keep_ref[...] = jnp.where(is_core, odd, even).astype(BF16)
    send_ref[...] = jnp.where(is_core, even, odd).astype(BF16)


def pack_kernel(capacity, at_ref, keep_ref, got_ref, out_ref):
    low, high = windows(at_ref, keep_ref, got_ref)
    extra = capacity - keep_ref.shape[2]
    if extra == keep_ref.shape[2]:
        main, tail = low, high
    else:
        high = pltpu.roll(high, extra, 1)
        spill = lax.broadcasted_iota(jnp.int32, high.shape, 1) < extra
        main = low + jnp.where(spill, 0.0, high)
        tail = jnp.where(spill, high, 0.0)
    store_packed(main, tail, extra, out_ref)


def combine_kernel(capacity, pooled, rows_ref, rank_ref, load_ref, out_ref, square_ref, kept_ref):
    cols, total = out_ref.shape
    chips = rows_ref.shape[0]
    extra = capacity - LANES
    groups = LANES // extra
    each = cols // groups
    row = lax.broadcasted_iota(jnp.int32, (2 * LANES, total), 0)
    slot = jnp.where(row < LANES, row, LANES + (row - LANES) % extra).astype(F32).astype(BF16)
    col = lax.broadcasted_iota(jnp.int32, (cols, LANES), 0)
    lane = lax.broadcasted_iota(jnp.int32, (cols, LANES), 1)
    own = (col // each) == (lane // extra)
    one = jnp.ones((), BF16)
    zero = jnp.zeros((), BF16)
    group = rank_ref.shape[0]
    half = capacity // 2
    if pooled:
        kept, _, _ = shed(load_ref[...], capacity)
        kept_ref[...] = jnp.concatenate([kept] * (total // LANES), axis=1)

    def step(s, acc):
        low = rank_ref[pl.ds(2 * s, 1), :]
        high = rank_ref[pl.ds(2 * s + 1, 1), :]
        if pooled:
            kept_low = kept_ref[pl.ds(2 * s, 1), :]
            kept_high = kept_ref[pl.ds(2 * s + 1, 1), :]
            before = lax.rem(2 * s - 2 + group, group)
            after = lax.rem(2 * s + 3, group)
            left = rank_ref[pl.ds(before, 1), :]
            right = rank_ref[pl.ds(after, 1), :]
            left = jnp.where(left < kept_ref[pl.ds(before, 1), :], -1.0, kept_low + left - half)
            right = jnp.where(
                right < kept_ref[pl.ds(after, 1), :],
                -1.0,
                capacity - 1.0 - (kept_high + right - half),
            )
            low = jnp.where(low < kept_low, low, -1.0)
            high = jnp.where(high < kept_high, high, -1.0)
        high = jnp.where(high < 0.0, -1.0, capacity - 1.0 - high)
        hit = (slot == low.astype(BF16)) | (slot == high.astype(BF16))
        if pooled:
            hit = hit | (slot == left.astype(BF16)) | (slot == right.astype(BF16))
        pick = jnp.where(hit, one, zero)
        block = rows_ref[s].astype(F32)
        tail = jnp.concatenate([block[cols:]] * groups, axis=0)
        tail = jnp.where(own, tail, 0.0)
        left = jnp.concatenate([block[:cols], tail], axis=1).astype(BF16)
        return acc + jnp.dot(left, pick, preferred_element_type=F32)

    out = lax.fori_loop(0, chips, step, jnp.zeros((cols, total), F32), unroll=4)
    out_ref[...] = out
    square_ref[...] = jnp.sum(out * out, axis=0, keepdims=True)


def spread_kernel(mine_ref, other_ref, out_ref):
    square = mine_ref[...] + other_ref[...]
    chips, lines, _ = out_ref.shape
    for i in range(lines):
        out_ref[:, i : i + 1, :] = jnp.broadcast_to(
            square[None, :, i * LANES : (i + 1) * LANES], (chips, 1, LANES)
        ).astype(BF16)


def finish_kernel(width, at_ref, squares_ref, mixed_ref, gain_ref, out_ref):
    sums = jnp.sum(squares_ref[...].astype(F32), axis=0)
    mean = jnp.concatenate([sums[i : i + 1] for i in range(sums.shape[0])], axis=1) / width
    cols = mixed_ref.shape[0]
    each = LANES // cols
    me = at_ref[0]
    gain = jnp.broadcast_to(gain_ref[pl.ds(me // each, 1), :], (LANES, LANES))
    gain = pltpu.roll(gain, (each - me % each) % each * cols, 1)
    gain = jnp.transpose(gain)[:cols, :1]
    out_ref[...] = (mixed_ref[...] * lax.rsqrt(mean + EPSILON) * gain).astype(BF16)


def shards(tokens, routes, gate_weights, norm_gain, final_gain, w_gate, w_up, w_down):
    per_dev, width = tokens.shape
    topk = routes.shape[1]
    group = lax.axis_size(EP)
    chips = group // 2
    cols = width // group
    total = per_dev * group
    most = 2 * group
    me = lax.axis_index(EP)
    core = lax.axis_index("core")
    odd = lax.axis_index("zl")
    at = jnp.stack([me, core, odd]).astype(jnp.int32)

    payload = pl.pallas_call(
        payload_kernel,
        out_shape=jax.ShapeDtypeStruct((per_dev, width + LANES), BF16),
        scratch_shapes=[pltpu.VMEM((LANES, LANES), F32)],
    )(tokens, jnp.transpose(routes), jnp.transpose(gate_weights), norm_gain[None, :])

    zigzag = []
    for chip in range(chips):
        zigzag.append((chip * 2, ((chip + 1) % chips) * 2))
        zigzag.append((chip * 2 + 1, ((chip - 1) % chips) * 2 + 1))
    swap = [(0, 1), (1, 0)]
    own = lax.all_gather(payload, "zh", axis=0, tiled=True)
    near = lax.ppermute(own, EP, zigzag)
    own_pair = lax.ppermute(own, "core", swap)
    near_pair = lax.ppermute(near, "core", swap)
    pieces = (own, own_pair, near, near_pair)
    part = own.shape[0]

    window = jax.ShapeDtypeStruct((chips, cols, LANES), BF16)
    sizes = (most * 5 // 4, most * 3 // 2, most * 2)
    rank, keep, send, load, level = pl.pallas_call(
        functools.partial(experts_kernel, topk, sizes),
        in_specs=[SMEM] + [VMEM] * CLASSES + [HBM] * 3,
        out_specs=[VMEM, VMEM, VMEM, VMEM, SMEM],
        out_shape=[
            jax.ShapeDtypeStruct((group, total), F32),
            window,
            window,
            jax.ShapeDtypeStruct((group, LANES), F32),
            jax.ShapeDtypeStruct((1,), jnp.int32),
        ],
        scratch_shapes=[
            pltpu.VMEM(w_gate.shape[1:], BF16),
            pltpu.VMEM(w_up.shape[1:], BF16),
            pltpu.VMEM(w_down.shape[1:], BF16),
            pltpu.SemaphoreType.DMA((3,)),
        ],
        compiler_params=pltpu.CompilerParams(vmem_limit_bytes=50 << 20),
    )(at, *pieces, w_gate, w_up, w_down)
    got = lax.ppermute(send, "core", swap)
    lines = total // LANES

    right = [(i, (i + 2) % group) for i in range(group)]
    left = [(i, (i - 2) % group) for i in range(group)]
    small = pltpu.CompilerParams(vmem_limit_bytes=16 << 20)

    def branch(capacity, pooled):
        packed = cols * capacity // LANES
        message = jax.ShapeDtypeStruct((chips, packed, LANES), BF16)
        spill = jax.ShapeDtypeStruct((chips * cols // 2, LANES), BF16)

        def run(at, keep, got, rank, load):
            if pooled:
                to_right, to_left = pl.pallas_call(
                    spill_kernel,
                    in_specs=[SMEM, VMEM, VMEM],
                    out_shape=[spill, spill],
                    compiler_params=small,
                )(at, keep, got)
                both = pl.pallas_call(
                    functools.partial(pooled_pack_kernel, capacity),
                    in_specs=[SMEM] + [VMEM] * 5,
                    out_shape=message,
                    compiler_params=small,
                )(at, keep, got, lax.ppermute(to_right, EP, right), lax.ppermute(to_left, EP, left), load)
            else:
                both = pl.pallas_call(
                    functools.partial(pack_kernel, capacity),
                    in_specs=[SMEM, VMEM, VMEM],
                    out_shape=message,
                    compiler_params=small,
                )(at, keep, got)
            returned = lax.all_to_all(both, CHIPS, split_axis=0, concat_axis=0, tiled=True)
            return pl.pallas_call(
                functools.partial(combine_kernel, capacity, pooled),
                in_specs=[VMEM] * 3,
                out_shape=[
                    jax.ShapeDtypeStruct((cols, total), F32),
                    jax.ShapeDtypeStruct((1, total), F32),
                ],
                scratch_shapes=[pltpu.VMEM((group, total), F32)],
                compiler_params=small,
            )(returned, rank, load)

        return run

    mixed, square = lax.switch(
        level[0],
        [branch(sizes[0], False), branch(sizes[1], False), branch(sizes[0], True), branch(sizes[2], False)],
        at, keep, got, rank, load,
    )

    spread = pl.pallas_call(
        spread_kernel,
        in_specs=[VMEM] * 2,
        out_shape=jax.ShapeDtypeStruct((chips, total // LANES, LANES), BF16),
        compiler_params=small,
    )(square, lax.ppermute(square, "core", swap))
    squares = lax.all_to_all(spread, CHIPS, split_axis=0, concat_axis=0, tiled=True)
    finished = pl.pallas_call(
        functools.partial(finish_kernel, width),
        in_specs=[SMEM] + [VMEM] * 3,
        out_shape=jax.ShapeDtypeStruct((cols, total), BF16),
        compiler_params=small,
    )(at, squares, mixed, final_gain.reshape(-1, LANES))
    return jnp.transpose(finished)


def solution(mesh):
    split = Mesh(mesh.devices.reshape(mesh.shape["grp"], 16, 2, 2), GRP_EP)
    return jax.shard_map(
        shards,
        mesh=split,
        in_specs=(
            P(GRP_EP, None),
            P(GRP_EP, None),
            P(GRP_EP, None),
            P(),
            P(),
            P(EP, None, None),
            P(EP, None, None),
            P(EP, None, None),
        ),
        out_specs=P("grp", EP),
        check_vma=False,
    )
```

```python
import functools

import jax
import jax.numpy as jnp
from jax import lax
from jax.experimental import pallas as pl
from jax.experimental.pallas import tpu as pltpu
from jax.sharding import Mesh
from jax.sharding import PartitionSpec as P

EP = ("zh", "zl", "core")
CHIPS = ("zh", "zl")
GRP_EP = ("grp", "zh", "zl", "core")
LANES = 128
CLASSES = 4
EPSILON = 1e-06
F32 = jnp.float32
BF16 = jnp.bfloat16

VMEM = pl.BlockSpec(memory_space=pltpu.VMEM)
SMEM = pl.BlockSpec(memory_space=pltpu.SMEM)
HBM = pl.BlockSpec(memory_space=pltpu.HBM)


def by_class(parts, is_core, is_odd):
    a, b, c, d = parts
    a, b, c, d = (
        jnp.where(is_core, b, a),
        jnp.where(is_core, a, b),
        jnp.where(is_core, d, c),
        jnp.where(is_core, c, d),
    )
    return (
        jnp.where(is_odd, c, a),
        jnp.where(is_odd, d, b),
        jnp.where(is_odd, a, c),
        jnp.where(is_odd, b, d),
    )


def payload_kernel(tokens_ref, routes_ref, gates_ref, gain_ref, out_ref, meta_ref):
    width = tokens_ref.shape[1]
    per_dev = tokens_ref.shape[0]
    topk = routes_ref.shape[0]
    values = tokens_ref[...].astype(F32)
    mean = jnp.mean(values * values, axis=1, keepdims=True)
    out_ref[:, :width] = (values * lax.rsqrt(mean + EPSILON) * gain_ref[...]).astype(BF16)
    gates = gates_ref[...]
    high = gates.astype(BF16).astype(F32)
    mid = (gates - high).astype(BF16).astype(F32)
    meta_ref[...] = jnp.zeros(meta_ref.shape, F32)
    meta_ref[0:topk, 0:per_dev] = routes_ref[...].astype(F32)
    meta_ref[topk : 2 * topk, 0:per_dev] = high
    meta_ref[2 * topk : 3 * topk, 0:per_dev] = mid
    meta_ref[3 * topk : 4 * topk, 0:per_dev] = gates - high - mid
    out_ref[:, width:] = jnp.transpose(meta_ref[...])[:per_dev, :].astype(BF16)


def shed(load, capacity):
    group = load.shape[0]
    even = lax.broadcasted_iota(jnp.int32, load.shape, 0) % 2 == 0
    at = lambda x, d: pltpu.roll(x, (-d) % group, 0)
    chip = load + jnp.where(even, at(load, 1), at(load, -1))
    half = capacity // 2
    over = jnp.where(chip > capacity, jnp.maximum(load - half, 0.0), 0.0)
    kept = load - over
    settled = jnp.where(even, kept + at(kept, 1) + at(over, -2) + at(over, 3), 0.0)
    return kept, chip, settled


def windows(at_ref, keep_ref, got_ref):
    is_core = at_ref[1] == 1
    chips, cols, slots = keep_ref.shape
    keep = keep_ref[...].astype(F32).reshape(chips * cols, slots)
    got = got_ref[...].astype(F32).reshape(chips * cols, slots)
    return jnp.where(is_core, got, keep), jnp.where(is_core, keep, got)


def spill_kernel(at_ref, keep_ref, got_ref, right_ref, left_ref):
    low, high = windows(at_ref, keep_ref, got_ref)
    rows = right_ref.shape[0]
    side = LANES // 2
    lane = lax.broadcasted_iota(jnp.int32, (rows, LANES), 1)
    right_ref[...] = jnp.where(
        lane >= side, low[:rows], pltpu.roll(low[rows:], side, 1)
    ).astype(BF16)
    left_ref[...] = jnp.where(
        lane < side, high[:rows], pltpu.roll(high[rows:], side, 1)
    ).astype(BF16)


def pooled_pack_kernel(capacity, at_ref, keep_ref, got_ref, right_ref, left_ref, load_ref, out_ref, took_ref):
    low, high = windows(at_ref, keep_ref, got_ref)
    chips, cols, slots = keep_ref.shape
    extra = capacity - slots
    half = capacity // 2
    load = load_ref[...]
    group = load.shape[0]
    kept, _, _ = shed(load, capacity)
    over = load - kept
    row = lax.broadcasted_iota(jnp.int32, load.shape, 0)
    first = at_ref[0] // 2 * 2
    came = pltpu.roll(over, 2, 0) + pltpu.roll(over, group - 3, 0)
    bit = jnp.where((row % 2 == 0) & (came > 0.0), jnp.left_shift(1, row % 32 // 2), 0)
    halves = [jnp.where(row // 32 == h, bit, 0) for h in range(group // 32)]
    for h, half_bits in enumerate(halves):
        took_ref[h] = jnp.max(jnp.sum(half_bits, axis=0, keepdims=True).astype(F32)).astype(jnp.int32)
    one = lambda x, e: jnp.max(jnp.where(row == (e + group) % group, x, 0.0)).astype(jnp.int32)
    kept_low, kept_high = one(kept, first), one(kept, first + 1)
    from_left, from_right = one(over, first - 2), one(over, first + 3)
    lane = lax.broadcasted_iota(jnp.int32, low.shape, 1)
    side = LANES // 2
    unfold = lambda ref: jnp.concatenate(
        [ref[...].astype(F32), pltpu.roll(ref[...].astype(F32), side, 1)], axis=0
    )
    low = jnp.where(lane < kept_low, low, 0.0)
    high = jnp.where(lane >= slots - kept_high, high, 0.0)
    left = unfold(right_ref)
    left = jnp.where((lane >= half) & (lane < half + from_left), left, 0.0)
    right = unfold(left_ref)
    top = slots - 1 - half
    right = jnp.where((lane <= top) & (lane > top - from_right), right, 0.0)
    high = pltpu.roll(high, extra, 1)
    left = pltpu.roll(left, (kept_low - half + slots) % slots, 1)
    right = pltpu.roll(right, (capacity - 1 - kept_high - top + slots) % slots, 1)
    main = low + jnp.where(lane >= extra, high, 0.0)
    main = main + jnp.where(lane >= kept_low, left, 0.0)
    main = main + jnp.where(lane >= extra - kept_high, right, 0.0)
    tail = jnp.where(lane < extra, high, 0.0)
    tail = tail + jnp.where(lane < kept_low, left, 0.0)
    tail = tail + jnp.where(lane < extra - kept_high, right, 0.0)
    store_packed(main, tail, extra, out_ref)


def store_packed(main, tail, extra, out_ref):
    chips, packed, slots = out_ref.shape
    cols = main.shape[0] // chips
    groups = slots // extra
    each = cols // groups
    out_ref[:, :cols, :] = main.reshape(chips, cols, slots).astype(BF16)
    tail = tail.reshape(chips, cols, slots)
    out = tail[:, :each].reshape(chips * each, slots)
    for g in range(1, groups):
        out = out + pltpu.roll(
            tail[:, g * each : (g + 1) * each].reshape(chips * each, slots), g * extra, 1
        )
    out_ref[:, cols:, :] = out.reshape(chips, each, slots).astype(BF16)


def experts_kernel(
    topk, sizes, at_ref, a_ref, b_ref, c_ref, d_ref, wg_hbm, wu_hbm, wd_hbm,
    rank_ref, keep_ref, send_ref, load_ref, level_ref, wg_ref, wu_ref, wd_ref, sems,
):
    copies = [
        pltpu.make_async_copy(src.at[0], dst, sems.at[i])
        for i, (src, dst) in enumerate(((wg_hbm, wg_ref), (wu_hbm, wu_ref), (wd_hbm, wd_ref)))
    ]
    copies[0].start()
    copies[1].start()
    width = wg_ref.shape[0]
    is_core = at_ref[1] == 1
    is_odd = at_ref[2] == 1
    me = at_ref[0].astype(F32)
    group, total = rank_ref.shape
    chips, cols, slots = keep_ref.shape
    per_dev = total // group
    part = a_ref.shape[0]
    outer = part // per_dev
    refs = (a_ref, b_ref, c_ref, d_ref)
    meta = by_class([r[:, width:].astype(F32) for r in refs], is_core, is_odd)
    grouped = jnp.concatenate([jnp.transpose(m) for m in meta], axis=1)
    rows = jnp.concatenate(
        [m[i * per_dev : (i + 1) * per_dev] for i in range(outer) for m in meta], axis=0
    )
    ordered = jnp.concatenate(
        [jnp.transpose(rows[i * LANES : (i + 1) * LANES]) for i in range(total // LANES)], axis=1
    )
    expert = lax.broadcasted_iota(jnp.int32, (group, total), 0).astype(F32)
    match = jnp.zeros((group, total), F32)
    for k in range(topk):
        match = match + jnp.where(ordered[k : k + 1, :] == expert, 1.0, 0.0)
    index = lax.broadcasted_iota(jnp.int32, (total, total), 0)
    at = lax.broadcasted_iota(jnp.int32, (total, total), 1)
    place = at % part // per_dev * (per_dev * CLASSES) + at // part * per_dev + at % per_dev
    counts = match.astype(BF16)
    rank = jnp.dot(
        counts, jnp.where(index < at, 1.0, 0.0).astype(BF16), preferred_element_type=F32
    )
    rank_ref[...] = jnp.where(match > 0.0, rank, -1.0)
    moved = jnp.dot(
        counts, jnp.where(index < place, 1.0, 0.0).astype(BF16), preferred_element_type=F32
    )
    slot = jnp.sum(jnp.where(expert == me, moved, 0.0), axis=0, keepdims=True)
    slot = jnp.where(is_core, slots - 1 - slot, slot)
    gates = grouped[topk : 2 * topk] + grouped[2 * topk : 3 * topk] + grouped[3 * topk : 4 * topk]
    mine = jnp.zeros((1, total), F32)
    gate = jnp.zeros((1, total), F32)
    for k in range(topk):
        named = grouped[k : k + 1, :] == me
        mine = jnp.where(named, 1.0, mine)
        gate = jnp.where(named, gates[k : k + 1, :], gate)
    slot = jnp.where(mine > 0.0, slot, -1.0).astype(jnp.int32)
    gate = jnp.concatenate(
        by_class([gate[:, k * part : (k + 1) * part] for k in range(CLASSES)], is_core, is_odd), axis=1
    )
    slot = jnp.concatenate(
        by_class([slot[:, k * part : (k + 1) * part] for k in range(CLASSES)], is_core, is_odd), axis=1
    )
    load = jnp.broadcast_to(jnp.sum(match, axis=1, keepdims=True), (group, LANES))
    load_ref[...] = load
    kept, chip, settled = shed(load, sizes[0])
    most = jnp.max(chip).astype(jnp.int32)
    fits = (jnp.max(settled).astype(jnp.int32) <= sizes[0]).astype(jnp.int32)
    level_ref[0] = jnp.where(
        most <= sizes[0], 0, jnp.where(most <= sizes[1], 1, 3 - fits)
    ).astype(jnp.int32)

    hit = lax.broadcasted_iota(jnp.int32, (slots, total), 0) == slot
    pick = jnp.where(hit, 1.0, 0.0).astype(BF16)
    gate = jnp.sum(jnp.where(hit, gate, 0.0), axis=1, keepdims=True)
    picked = jnp.zeros((slots, width), F32)
    for k, ref in enumerate(refs):
        picked = picked + jnp.dot(
            pick[:, k * part : (k + 1) * part], ref[:, :width], preferred_element_type=F32
        )
    picked = picked.astype(BF16)
    copies[0].wait()
    copies[2].start()
    gate_val = jnp.dot(picked, wg_ref[...], preferred_element_type=F32)
    copies[1].wait()
    up_val = jnp.dot(picked, wu_ref[...], preferred_element_type=F32)
    act = (gate_val * jax.nn.sigmoid(gate_val) * up_val * gate).astype(BF16)
    copies[2].wait()
    result = jnp.dot(act, wd_ref[...], preferred_element_type=F32)
    result = jnp.transpose(result).reshape(chips, 2, cols, slots)
    even, odd = result[:, 0], result[:, 1]
    keep_ref[...] = jnp.where(is_core, odd, even).astype(BF16)
    send_ref[...] = jnp.where(is_core, even, odd).astype(BF16)


def pack_kernel(capacity, at_ref, keep_ref, got_ref, out_ref):
    low, high = windows(at_ref, keep_ref, got_ref)
    extra = capacity - keep_ref.shape[2]
    if extra == keep_ref.shape[2]:
        main, tail = low, high
    else:
        high = pltpu.roll(high, extra, 1)
        spill = lax.broadcasted_iota(jnp.int32, high.shape, 1) < extra
        main = low + jnp.where(spill, 0.0, high)
        tail = jnp.where(spill, high, 0.0)
    store_packed(main, tail, extra, out_ref)


def combine_kernel(capacity, pooled, took_ref, rows_ref, rank_ref, load_ref, out_ref, square_ref, kept_ref):
    cols, total = out_ref.shape
    chips = rows_ref.shape[0]
    extra = capacity - LANES
    groups = LANES // extra
    each = cols // groups
    row = lax.broadcasted_iota(jnp.int32, (2 * LANES, total), 0)
    slot = jnp.where(row < LANES, row, LANES + (row - LANES) % extra).astype(F32).astype(BF16)
    col = lax.broadcasted_iota(jnp.int32, (cols, LANES), 0)
    lane = lax.broadcasted_iota(jnp.int32, (cols, LANES), 1)
    own = (col // each) == (lane // extra)
    one = jnp.ones((), BF16)
    zero = jnp.zeros((), BF16)
    group = rank_ref.shape[0]
    half = capacity // 2
    if pooled:
        kept, _, _ = shed(load_ref[...], capacity)
        kept_ref[...] = jnp.concatenate([kept] * (total // LANES), axis=1)

    def add(s, acc, hit):
        pick = jnp.where(hit, one, zero)
        block = rows_ref[s].astype(F32)
        tail = jnp.concatenate([block[cols:]] * groups, axis=0)
        tail = jnp.where(own, tail, 0.0)
        left = jnp.concatenate([block[:cols], tail], axis=1).astype(BF16)
        return acc + jnp.dot(left, pick, preferred_element_type=F32)

    def keys(s):
        low = rank_ref[pl.ds(2 * s, 1), :]
        high = rank_ref[pl.ds(2 * s + 1, 1), :]
        if pooled:
            low = jnp.where(low < kept_ref[pl.ds(2 * s, 1), :], low, -1.0)
            high = jnp.where(high < kept_ref[pl.ds(2 * s + 1, 1), :], high, -1.0)
        high = jnp.where(high < 0.0, -1.0, capacity - 1.0 - high)
        return (slot == low.astype(BF16)) | (slot == high.astype(BF16))

    def step(s, acc):
        return add(s, acc, keys(s))

    out = lax.fori_loop(0, chips, step, jnp.zeros((cols, total), F32), unroll=8)
    if pooled:

        def more(s, acc):
            def surplus(acc):
                before = lax.rem(2 * s - 2 + group, group)
                after = lax.rem(2 * s + 3, group)
                left = rank_ref[pl.ds(before, 1), :]
                right = rank_ref[pl.ds(after, 1), :]
                left = jnp.where(
                    left < kept_ref[pl.ds(before, 1), :],
                    -1.0,
                    kept_ref[pl.ds(2 * s, 1), :] + left - half,
                )
                right = jnp.where(
                    right < kept_ref[pl.ds(after, 1), :],
                    -1.0,
                    capacity - 1.0 - (kept_ref[pl.ds(2 * s + 1, 1), :] + right - half),
                )
                return add(s, acc, (slot == left.astype(BF16)) | (slot == right.astype(BF16)))

            took = (took_ref[s // 16] >> (s % 16)) & 1
            return lax.cond(took == 1, surplus, lambda acc: acc, acc)

        out = lax.fori_loop(0, chips, more, out)
    out_ref[...] = out
    square_ref[...] = jnp.sum(out * out, axis=0, keepdims=True)


def spread_kernel(mine_ref, other_ref, out_ref):
    square = mine_ref[...] + other_ref[...]
    chips, lines, _ = out_ref.shape
    for i in range(lines):
        out_ref[:, i : i + 1, :] = jnp.broadcast_to(
            square[None, :, i * LANES : (i + 1) * LANES], (chips, 1, LANES)
        ).astype(BF16)


def finish_kernel(width, at_ref, squares_ref, mixed_ref, gain_ref, out_ref):
    sums = jnp.sum(squares_ref[...].astype(F32), axis=0)
    mean = jnp.concatenate([sums[i : i + 1] for i in range(sums.shape[0])], axis=1) / width
    cols = mixed_ref.shape[0]
    each = LANES // cols
    me = at_ref[0]
    gain = jnp.broadcast_to(gain_ref[pl.ds(me // each, 1), :], (LANES, LANES))
    gain = pltpu.roll(gain, (each - me % each) % each * cols, 1)
    gain = jnp.transpose(gain)[:cols, :1]
    out_ref[...] = (mixed_ref[...] * lax.rsqrt(mean + EPSILON) * gain).astype(BF16)


def shards(tokens, routes, gate_weights, norm_gain, final_gain, w_gate, w_up, w_down):
    per_dev, width = tokens.shape
    topk = routes.shape[1]
    group = lax.axis_size(EP)
    chips = group // 2
    cols = width // group
    total = per_dev * group
    most = 2 * group
    me = lax.axis_index(EP)
    core = lax.axis_index("core")
    odd = lax.axis_index("zl")
    at = jnp.stack([me, core, odd]).astype(jnp.int32)

    payload = pl.pallas_call(
        payload_kernel,
        out_shape=jax.ShapeDtypeStruct((per_dev, width + LANES), BF16),
        scratch_shapes=[pltpu.VMEM((LANES, LANES), F32)],
    )(tokens, jnp.transpose(routes), jnp.transpose(gate_weights), norm_gain[None, :])

    zigzag = []
    for chip in range(chips):
        zigzag.append((chip * 2, ((chip + 1) % chips) * 2))
        zigzag.append((chip * 2 + 1, ((chip - 1) % chips) * 2 + 1))
    swap = [(0, 1), (1, 0)]
    own = lax.all_gather(payload, "zh", axis=0, tiled=True)
    near = lax.ppermute(own, EP, zigzag)
    own_pair = lax.ppermute(own, "core", swap)
    near_pair = lax.ppermute(near, "core", swap)
    pieces = (own, own_pair, near, near_pair)
    part = own.shape[0]

    window = jax.ShapeDtypeStruct((chips, cols, LANES), BF16)
    sizes = (most * 5 // 4, most * 3 // 2, most * 2)
    rank, keep, send, load, level = pl.pallas_call(
        functools.partial(experts_kernel, topk, sizes),
        in_specs=[SMEM] + [VMEM] * CLASSES + [HBM] * 3,
        out_specs=[VMEM, VMEM, VMEM, VMEM, SMEM],
        out_shape=[
            jax.ShapeDtypeStruct((group, total), F32),
            window,
            window,
            jax.ShapeDtypeStruct((group, LANES), F32),
            jax.ShapeDtypeStruct((1,), jnp.int32),
        ],
        scratch_shapes=[
            pltpu.VMEM(w_gate.shape[1:], BF16),
            pltpu.VMEM(w_up.shape[1:], BF16),
            pltpu.VMEM(w_down.shape[1:], BF16),
            pltpu.SemaphoreType.DMA((3,)),
        ],
        compiler_params=pltpu.CompilerParams(vmem_limit_bytes=50 << 20),
    )(at, *pieces, w_gate, w_up, w_down)
    got = lax.ppermute(send, "core", swap)
    lines = total // LANES

    right = [(i, (i + 2) % group) for i in range(group)]
    left = [(i, (i - 2) % group) for i in range(group)]
    small = pltpu.CompilerParams(vmem_limit_bytes=16 << 20)

    def branch(capacity, pooled):
        packed = cols * capacity // LANES
        message = jax.ShapeDtypeStruct((chips, packed, LANES), BF16)
        spill = jax.ShapeDtypeStruct((chips * cols // 2, LANES), BF16)

        def run(at, keep, got, rank, load):
            if pooled:
                to_right, to_left = pl.pallas_call(
                    spill_kernel,
                    in_specs=[SMEM, VMEM, VMEM],
                    out_shape=[spill, spill],
                    compiler_params=small,
                )(at, keep, got)
                both, took = pl.pallas_call(
                    functools.partial(pooled_pack_kernel, capacity),
                    in_specs=[SMEM] + [VMEM] * 5,
                    out_specs=[VMEM, SMEM],
                    out_shape=[message, jax.ShapeDtypeStruct((group // 32,), jnp.int32)],
                    compiler_params=small,
                )(at, keep, got, lax.ppermute(to_right, EP, right), lax.ppermute(to_left, EP, left), load)
            else:
                took = at
                both = pl.pallas_call(
                    functools.partial(pack_kernel, capacity),
                    in_specs=[SMEM, VMEM, VMEM],
                    out_shape=message,
                    compiler_params=small,
                )(at, keep, got)
            returned = lax.all_to_all(both, CHIPS, split_axis=0, concat_axis=0, tiled=True)
            return pl.pallas_call(
                functools.partial(combine_kernel, capacity, pooled),
                in_specs=[SMEM] + [VMEM] * 3,
                out_shape=[
                    jax.ShapeDtypeStruct((cols, total), F32),
                    jax.ShapeDtypeStruct((1, total), F32),
                ],
                scratch_shapes=[pltpu.VMEM((group, total), F32)],
                compiler_params=small,
            )(took, returned, rank, load)

        return run

    mixed, square = lax.switch(
        level[0],
        [branch(sizes[0], False), branch(sizes[1], False), branch(sizes[0], True), branch(sizes[2], False)],
        at, keep, got, rank, load,
    )

    spread = pl.pallas_call(
        spread_kernel,
        in_specs=[VMEM] * 2,
        out_shape=jax.ShapeDtypeStruct((chips, total // LANES, LANES), BF16),
        compiler_params=small,
    )(square, lax.ppermute(square, "core", swap))
    squares = lax.all_to_all(spread, CHIPS, split_axis=0, concat_axis=0, tiled=True)
    finished = pl.pallas_call(
        functools.partial(finish_kernel, width),
        in_specs=[SMEM] + [VMEM] * 3,
        out_shape=jax.ShapeDtypeStruct((cols, total), BF16),
        compiler_params=small,
    )(at, squares, mixed, final_gain.reshape(-1, LANES))
    return jnp.transpose(finished)


def solution(mesh):
    split = Mesh(mesh.devices.reshape(mesh.shape["grp"], 16, 2, 2), GRP_EP)
    return jax.shard_map(
        shards,
        mesh=split,
        in_specs=(
            P(GRP_EP, None),
            P(GRP_EP, None),
            P(GRP_EP, None),
            P(),
            P(),
            P(EP, None, None),
            P(EP, None, None),
            P(EP, None, None),
        ),
        out_specs=P("grp", EP),
        check_vma=False,
    )
```

```python
import functools

import jax
import jax.numpy as jnp
from jax import lax
from jax.experimental import pallas as pl
from jax.experimental.pallas import tpu as pltpu
from jax.sharding import Mesh
from jax.sharding import PartitionSpec as P

EP = ("zh", "zl", "core")
CHIPS = ("zh", "zl")
GRP_EP = ("grp", "zh", "zl", "core")
LANES = 128
CLASSES = 4
CHUNKS = 4
EPSILON = 1e-06
F32 = jnp.float32
BF16 = jnp.bfloat16

VMEM = pl.BlockSpec(memory_space=pltpu.VMEM)
SMEM = pl.BlockSpec(memory_space=pltpu.SMEM)
HBM = pl.BlockSpec(memory_space=pltpu.HBM)


def by_class(parts, is_core, is_odd):
    a, b, c, d = parts
    a, b, c, d = (
        jnp.where(is_core, b, a),
        jnp.where(is_core, a, b),
        jnp.where(is_core, d, c),
        jnp.where(is_core, c, d),
    )
    return (
        jnp.where(is_odd, c, a),
        jnp.where(is_odd, d, b),
        jnp.where(is_odd, a, c),
        jnp.where(is_odd, b, d),
    )


def payload_kernel(tokens_ref, routes_ref, gates_ref, gain_ref, out_ref, meta_ref):
    width = tokens_ref.shape[1]
    per_dev = tokens_ref.shape[0]
    topk = routes_ref.shape[0]
    values = tokens_ref[...].astype(F32)
    mean = jnp.mean(values * values, axis=1, keepdims=True)
    out_ref[:, :width] = (values * lax.rsqrt(mean + EPSILON) * gain_ref[...]).astype(BF16)
    gates = gates_ref[...]
    high = gates.astype(BF16).astype(F32)
    mid = (gates - high).astype(BF16).astype(F32)
    meta_ref[...] = jnp.zeros(meta_ref.shape, F32)
    meta_ref[0:topk, 0:per_dev] = routes_ref[...].astype(F32)
    meta_ref[topk : 2 * topk, 0:per_dev] = high
    meta_ref[2 * topk : 3 * topk, 0:per_dev] = mid
    meta_ref[3 * topk : 4 * topk, 0:per_dev] = gates - high - mid
    out_ref[:, width:] = jnp.transpose(meta_ref[...])[:per_dev, :].astype(BF16)


def shed(load, capacity):
    group = load.shape[0]
    even = lax.broadcasted_iota(jnp.int32, load.shape, 0) % 2 == 0
    at = lambda x, d: pltpu.roll(x, (-d) % group, 0)
    chip = load + jnp.where(even, at(load, 1), at(load, -1))
    half = capacity // 2
    over = jnp.where(chip > capacity, jnp.maximum(load - half, 0.0), 0.0)
    kept = load - over
    settled = jnp.where(even, kept + at(kept, 1) + at(over, -2) + at(over, 3), 0.0)
    return kept, chip, settled


def windows(at_ref, keep_ref, got_ref):
    is_core = at_ref[1] == 1
    chips, cols, slots = keep_ref.shape
    keep = keep_ref[...].astype(F32).reshape(chips * cols, slots)
    got = got_ref[...].astype(F32).reshape(chips * cols, slots)
    return jnp.where(is_core, got, keep), jnp.where(is_core, keep, got)


def spill_kernel(at_ref, keep_ref, got_ref, right_ref, left_ref):
    low, high = windows(at_ref, keep_ref, got_ref)
    rows = right_ref.shape[0]
    side = LANES // 2
    lane = lax.broadcasted_iota(jnp.int32, (rows, LANES), 1)
    right_ref[...] = jnp.where(
        lane >= side, low[:rows], pltpu.roll(low[rows:], side, 1)
    ).astype(BF16)
    left_ref[...] = jnp.where(
        lane < side, high[:rows], pltpu.roll(high[rows:], side, 1)
    ).astype(BF16)


def pooled_pack_kernel(capacity, at_ref, keep_ref, got_ref, right_ref, left_ref, load_ref, out_ref, took_ref):
    low, high = windows(at_ref, keep_ref, got_ref)
    chips, cols, slots = keep_ref.shape
    extra = capacity - slots
    half = capacity // 2
    load = load_ref[...]
    group = load.shape[0]
    kept, _, _ = shed(load, capacity)
    over = load - kept
    row = lax.broadcasted_iota(jnp.int32, load.shape, 0)
    first = at_ref[0] // 2 * 2
    came = pltpu.roll(over, 2, 0) + pltpu.roll(over, group - 3, 0)
    bit = jnp.where((row % 2 == 0) & (came > 0.0), jnp.left_shift(1, row % 32 // 2), 0)
    halves = [jnp.where(row // 32 == h, bit, 0) for h in range(group // 32)]
    for h, half_bits in enumerate(halves):
        took_ref[h] = jnp.max(jnp.sum(half_bits, axis=0, keepdims=True).astype(F32)).astype(jnp.int32)
    one = lambda x, e: jnp.max(jnp.where(row == (e + group) % group, x, 0.0)).astype(jnp.int32)
    kept_low, kept_high = one(kept, first), one(kept, first + 1)
    from_left, from_right = one(over, first - 2), one(over, first + 3)
    lane = lax.broadcasted_iota(jnp.int32, low.shape, 1)
    side = LANES // 2
    unfold = lambda ref: jnp.concatenate(
        [ref[...].astype(F32), pltpu.roll(ref[...].astype(F32), side, 1)], axis=0
    )
    low = jnp.where(lane < kept_low, low, 0.0)
    high = jnp.where(lane >= slots - kept_high, high, 0.0)
    left = unfold(right_ref)
    left = jnp.where((lane >= half) & (lane < half + from_left), left, 0.0)
    right = unfold(left_ref)
    top = slots - 1 - half
    right = jnp.where((lane <= top) & (lane > top - from_right), right, 0.0)
    high = pltpu.roll(high, extra, 1)
    left = pltpu.roll(left, (kept_low - half + slots) % slots, 1)
    right = pltpu.roll(right, (capacity - 1 - kept_high - top + slots) % slots, 1)
    main = low + jnp.where(lane >= extra, high, 0.0)
    main = main + jnp.where(lane >= kept_low, left, 0.0)
    main = main + jnp.where(lane >= extra - kept_high, right, 0.0)
    tail = jnp.where(lane < extra, high, 0.0)
    tail = tail + jnp.where(lane < kept_low, left, 0.0)
    tail = tail + jnp.where(lane < extra - kept_high, right, 0.0)
    store_packed(main, tail, extra, out_ref)


def store_packed(main, tail, extra, out_ref):
    chips, packed, slots = out_ref.shape
    cols = main.shape[0] // chips
    groups = slots // extra
    each = cols // groups
    out_ref[:, :cols, :] = main.reshape(chips, cols, slots).astype(BF16)
    tail = tail.reshape(chips, cols, slots)
    out = tail[:, :each].reshape(chips * each, slots)
    for g in range(1, groups):
        out = out + pltpu.roll(
            tail[:, g * each : (g + 1) * each].reshape(chips * each, slots), g * extra, 1
        )
    out_ref[:, cols:, :] = out.reshape(chips, each, slots).astype(BF16)


def experts_kernel(
    topk, sizes, at_ref, a_ref, b_ref, c_ref, d_ref, wg_hbm, wu_hbm, wd_hbm,
    rank_ref, keep_ref, send_ref, load_ref, level_ref, wg_ref, wu_ref, wd_ref, sems,
):
    copies = []
    for i, (src, dst) in enumerate(((wg_hbm, wg_ref), (wu_hbm, wu_ref), (wd_hbm, wd_ref))):
        step = dst.shape[0] // CHUNKS
        copies.append(
            [
                pltpu.make_async_copy(
                    src.at[0, pl.ds(c * step, step)], dst.at[pl.ds(c * step, step)], sems.at[i, c]
                )
                for c in range(CHUNKS)
            ]
        )
    for copy in sum(copies, []):
        copy.start()
    width = wg_ref.shape[0]
    is_core = at_ref[1] == 1
    is_odd = at_ref[2] == 1
    me = at_ref[0].astype(F32)
    group, total = rank_ref.shape
    chips, cols, slots = keep_ref.shape
    per_dev = total // group
    part = a_ref.shape[0]
    outer = part // per_dev
    refs = (a_ref, b_ref, c_ref, d_ref)
    meta = by_class([r[:, width:].astype(F32) for r in refs], is_core, is_odd)
    grouped = jnp.concatenate([jnp.transpose(m) for m in meta], axis=1)
    rows = jnp.concatenate(
        [m[i * per_dev : (i + 1) * per_dev] for i in range(outer) for m in meta], axis=0
    )
    ordered = jnp.concatenate(
        [jnp.transpose(rows[i * LANES : (i + 1) * LANES]) for i in range(total // LANES)], axis=1
    )
    expert = lax.broadcasted_iota(jnp.int32, (group, total), 0).astype(F32)
    match = jnp.zeros((group, total), F32)
    for k in range(topk):
        match = match + jnp.where(ordered[k : k + 1, :] == expert, 1.0, 0.0)
    index = lax.broadcasted_iota(jnp.int32, (total, total), 0)
    at = lax.broadcasted_iota(jnp.int32, (total, total), 1)
    place = at % part // per_dev * (per_dev * CLASSES) + at // part * per_dev + at % per_dev
    counts = match.astype(BF16)
    rank = jnp.dot(
        counts, jnp.where(index < at, 1.0, 0.0).astype(BF16), preferred_element_type=F32
    )
    rank_ref[...] = jnp.where(match > 0.0, rank, -1.0)
    moved = jnp.dot(
        counts, jnp.where(index < place, 1.0, 0.0).astype(BF16), preferred_element_type=F32
    )
    slot = jnp.sum(jnp.where(expert == me, moved, 0.0), axis=0, keepdims=True)
    slot = jnp.where(is_core, slots - 1 - slot, slot)
    gates = grouped[topk : 2 * topk] + grouped[2 * topk : 3 * topk] + grouped[3 * topk : 4 * topk]
    mine = jnp.zeros((1, total), F32)
    gate = jnp.zeros((1, total), F32)
    for k in range(topk):
        named = grouped[k : k + 1, :] == me
        mine = jnp.where(named, 1.0, mine)
        gate = jnp.where(named, gates[k : k + 1, :], gate)
    slot = jnp.where(mine > 0.0, slot, -1.0).astype(jnp.int32)
    gate = jnp.concatenate(
        by_class([gate[:, k * part : (k + 1) * part] for k in range(CLASSES)], is_core, is_odd), axis=1
    )
    slot = jnp.concatenate(
        by_class([slot[:, k * part : (k + 1) * part] for k in range(CLASSES)], is_core, is_odd), axis=1
    )
    load = jnp.broadcast_to(jnp.sum(match, axis=1, keepdims=True), (group, LANES))
    load_ref[...] = load
    kept, chip, settled = shed(load, sizes[0])
    most = jnp.max(chip).astype(jnp.int32)
    fits = (jnp.max(settled).astype(jnp.int32) <= sizes[0]).astype(jnp.int32)
    level_ref[0] = jnp.where(
        most <= sizes[0], 0, jnp.where(most <= sizes[1], 1, 3 - fits)
    ).astype(jnp.int32)

    hit = lax.broadcasted_iota(jnp.int32, (slots, total), 0) == slot
    pick = jnp.where(hit, 1.0, 0.0).astype(BF16)
    gate = jnp.sum(jnp.where(hit, gate, 0.0), axis=1, keepdims=True)
    picked = jnp.zeros((slots, width), F32)
    for k, ref in enumerate(refs):
        picked = picked + jnp.dot(
            pick[:, k * part : (k + 1) * part], ref[:, :width], preferred_element_type=F32
        )
    picked = picked.astype(BF16)
    for copy in copies[0]:
        copy.wait()
    gate_val = jnp.dot(picked, wg_ref[...], preferred_element_type=F32)
    for copy in copies[1]:
        copy.wait()
    up_val = jnp.dot(picked, wu_ref[...], preferred_element_type=F32)
    act = (gate_val * jax.nn.sigmoid(gate_val) * up_val * gate).astype(BF16)
    for copy in copies[2]:
        copy.wait()
    result = jnp.dot(act, wd_ref[...], preferred_element_type=F32)
    result = jnp.transpose(result).reshape(chips, 2, cols, slots)
    even, odd = result[:, 0], result[:, 1]
    keep_ref[...] = jnp.where(is_core, odd, even).astype(BF16)
    send_ref[...] = jnp.where(is_core, even, odd).astype(BF16)


def pack_kernel(capacity, at_ref, keep_ref, got_ref, out_ref):
    low, high = windows(at_ref, keep_ref, got_ref)
    extra = capacity - keep_ref.shape[2]
    if extra == keep_ref.shape[2]:
        main, tail = low, high
    else:
        high = pltpu.roll(high, extra, 1)
        spill = lax.broadcasted_iota(jnp.int32, high.shape, 1) < extra
        main = low + jnp.where(spill, 0.0, high)
        tail = jnp.where(spill, high, 0.0)
    store_packed(main, tail, extra, out_ref)


def combine_kernel(capacity, pooled, took_ref, rows_ref, rank_ref, load_ref, out_ref, square_ref, kept_ref):
    cols, total = out_ref.shape
    chips = rows_ref.shape[0]
    extra = capacity - LANES
    groups = LANES // extra
    each = cols // groups
    row = lax.broadcasted_iota(jnp.int32, (2 * LANES, total), 0)
    slot = jnp.where(row < LANES, row, LANES + (row - LANES) % extra).astype(F32).astype(BF16)
    col = lax.broadcasted_iota(jnp.int32, (cols, LANES), 0)
    lane = lax.broadcasted_iota(jnp.int32, (cols, LANES), 1)
    own = (col // each) == (lane // extra)
    one = jnp.ones((), BF16)
    zero = jnp.zeros((), BF16)
    group = rank_ref.shape[0]
    half = capacity // 2
    if pooled:
        kept, _, _ = shed(load_ref[...], capacity)
        kept_ref[...] = jnp.concatenate([kept] * (total // LANES), axis=1)

    def add(s, acc, hit):
        pick = jnp.where(hit, one, zero)
        block = rows_ref[s].astype(F32)
        tail = jnp.concatenate([block[cols:]] * groups, axis=0)
        tail = jnp.where(own, tail, 0.0)
        left = jnp.concatenate([block[:cols], tail], axis=1).astype(BF16)
        return acc + jnp.dot(left, pick, preferred_element_type=F32)

    def keys(s):
        low = rank_ref[pl.ds(2 * s, 1), :]
        high = rank_ref[pl.ds(2 * s + 1, 1), :]
        if pooled:
            low = jnp.where(low < kept_ref[pl.ds(2 * s, 1), :], low, -1.0)
            high = jnp.where(high < kept_ref[pl.ds(2 * s + 1, 1), :], high, -1.0)
        high = jnp.where(high < 0.0, -1.0, capacity - 1.0 - high)
        return (slot == low.astype(BF16)) | (slot == high.astype(BF16))

    def step(s, acc):
        return add(s, acc, keys(s))

    out = lax.fori_loop(0, chips, step, jnp.zeros((cols, total), F32), unroll=4)
    if pooled:

        def more(s, acc):
            def surplus(acc):
                before = lax.rem(2 * s - 2 + group, group)
                after = lax.rem(2 * s + 3, group)
                left = rank_ref[pl.ds(before, 1), :]
                right = rank_ref[pl.ds(after, 1), :]
                left = jnp.where(
                    left < kept_ref[pl.ds(before, 1), :],
                    -1.0,
                    kept_ref[pl.ds(2 * s, 1), :] + left - half,
                )
                right = jnp.where(
                    right < kept_ref[pl.ds(after, 1), :],
                    -1.0,
                    capacity - 1.0 - (kept_ref[pl.ds(2 * s + 1, 1), :] + right - half),
                )
                return add(s, acc, (slot == left.astype(BF16)) | (slot == right.astype(BF16)))

            took = (took_ref[s // 16] >> (s % 16)) & 1
            return lax.cond(took == 1, surplus, lambda acc: acc, acc)

        out = lax.fori_loop(0, chips, more, out)
    out_ref[...] = out
    square_ref[...] = jnp.sum(out * out, axis=0, keepdims=True)


def spread_kernel(mine_ref, other_ref, out_ref):
    square = mine_ref[...] + other_ref[...]
    chips, lines, _ = out_ref.shape
    for i in range(lines):
        out_ref[:, i : i + 1, :] = jnp.broadcast_to(
            square[None, :, i * LANES : (i + 1) * LANES], (chips, 1, LANES)
        ).astype(BF16)


def finish_kernel(width, at_ref, squares_ref, mixed_ref, gain_ref, out_ref):
    sums = jnp.sum(squares_ref[...].astype(F32), axis=0)
    mean = jnp.concatenate([sums[i : i + 1] for i in range(sums.shape[0])], axis=1) / width
    cols = mixed_ref.shape[0]
    each = LANES // cols
    me = at_ref[0]
    gain = jnp.broadcast_to(gain_ref[pl.ds(me // each, 1), :], (LANES, LANES))
    gain = pltpu.roll(gain, (each - me % each) % each * cols, 1)
    gain = jnp.transpose(gain)[:cols, :1]
    out_ref[...] = (mixed_ref[...] * lax.rsqrt(mean + EPSILON) * gain).astype(BF16)


def shards(tokens, routes, gate_weights, norm_gain, final_gain, w_gate, w_up, w_down):
    per_dev, width = tokens.shape
    topk = routes.shape[1]
    group = lax.axis_size(EP)
    chips = group // 2
    cols = width // group
    total = per_dev * group
    most = 2 * group
    me = lax.axis_index(EP)
    core = lax.axis_index("core")
    odd = lax.axis_index("zl")
    at = jnp.stack([me, core, odd]).astype(jnp.int32)

    payload = pl.pallas_call(
        payload_kernel,
        out_shape=jax.ShapeDtypeStruct((per_dev, width + LANES), BF16),
        scratch_shapes=[pltpu.VMEM((LANES, LANES), F32)],
    )(tokens, jnp.transpose(routes), jnp.transpose(gate_weights), norm_gain[None, :])

    zigzag = []
    for chip in range(chips):
        zigzag.append((chip * 2, ((chip + 1) % chips) * 2))
        zigzag.append((chip * 2 + 1, ((chip - 1) % chips) * 2 + 1))
    swap = [(0, 1), (1, 0)]
    own = lax.all_gather(payload, "zh", axis=0, tiled=True)
    near = lax.ppermute(own, EP, zigzag)
    own_pair = lax.ppermute(own, "core", swap)
    near_pair = lax.ppermute(near, "core", swap)
    pieces = (own, own_pair, near, near_pair)
    part = own.shape[0]

    window = jax.ShapeDtypeStruct((chips, cols, LANES), BF16)
    sizes = (most * 5 // 4, most * 3 // 2, most * 2)
    rank, keep, send, load, level = pl.pallas_call(
        functools.partial(experts_kernel, topk, sizes),
        in_specs=[SMEM] + [VMEM] * CLASSES + [HBM] * 3,
        out_specs=[VMEM, VMEM, VMEM, VMEM, SMEM],
        out_shape=[
            jax.ShapeDtypeStruct((group, total), F32),
            window,
            window,
            jax.ShapeDtypeStruct((group, LANES), F32),
            jax.ShapeDtypeStruct((1,), jnp.int32),
        ],
        scratch_shapes=[
            pltpu.VMEM(w_gate.shape[1:], BF16),
            pltpu.VMEM(w_up.shape[1:], BF16),
            pltpu.VMEM(w_down.shape[1:], BF16),
            pltpu.SemaphoreType.DMA((3, CHUNKS)),
        ],
        compiler_params=pltpu.CompilerParams(vmem_limit_bytes=50 << 20),
    )(at, *pieces, w_gate, w_up, w_down)
    got = lax.ppermute(send, "core", swap)
    lines = total // LANES

    right = [(i, (i + 2) % group) for i in range(group)]
    left = [(i, (i - 2) % group) for i in range(group)]
    small = pltpu.CompilerParams(vmem_limit_bytes=16 << 20)

    def branch(capacity, pooled):
        packed = cols * capacity // LANES
        message = jax.ShapeDtypeStruct((chips, packed, LANES), BF16)
        spill = jax.ShapeDtypeStruct((chips * cols // 2, LANES), BF16)

        def run(at, keep, got, rank, load):
            if pooled:
                to_right, to_left = pl.pallas_call(
                    spill_kernel,
                    in_specs=[SMEM, VMEM, VMEM],
                    out_shape=[spill, spill],
                    compiler_params=small,
                )(at, keep, got)
                both, took = pl.pallas_call(
                    functools.partial(pooled_pack_kernel, capacity),
                    in_specs=[SMEM] + [VMEM] * 5,
                    out_specs=[VMEM, SMEM],
                    out_shape=[message, jax.ShapeDtypeStruct((group // 32,), jnp.int32)],
                    compiler_params=small,
                )(at, keep, got, lax.ppermute(to_right, EP, right), lax.ppermute(to_left, EP, left), load)
            else:
                took = at
                both = pl.pallas_call(
                    functools.partial(pack_kernel, capacity),
                    in_specs=[SMEM, VMEM, VMEM],
                    out_shape=message,
                    compiler_params=small,
                )(at, keep, got)
            returned = lax.all_to_all(both, CHIPS, split_axis=0, concat_axis=0, tiled=True)
            return pl.pallas_call(
                functools.partial(combine_kernel, capacity, pooled),
                in_specs=[SMEM] + [VMEM] * 3,
                out_shape=[
                    jax.ShapeDtypeStruct((cols, total), F32),
                    jax.ShapeDtypeStruct((1, total), F32),
                ],
                scratch_shapes=[pltpu.VMEM((group, total), F32)],
                compiler_params=small,
            )(took, returned, rank, load)

        return run

    mixed, square = lax.switch(
        level[0],
        [branch(sizes[0], False), branch(sizes[1], False), branch(sizes[0], True), branch(sizes[2], False)],
        at, keep, got, rank, load,
    )

    spread = pl.pallas_call(
        spread_kernel,
        in_specs=[VMEM] * 2,
        out_shape=jax.ShapeDtypeStruct((chips, total // LANES, LANES), BF16),
        compiler_params=small,
    )(square, lax.ppermute(square, "core", swap))
    squares = lax.all_to_all(spread, CHIPS, split_axis=0, concat_axis=0, tiled=True)
    finished = pl.pallas_call(
        functools.partial(finish_kernel, width),
        in_specs=[SMEM] + [VMEM] * 3,
        out_shape=jax.ShapeDtypeStruct((cols, total), BF16),
        compiler_params=small,
    )(at, squares, mixed, final_gain.reshape(-1, LANES))
    return jnp.transpose(finished)


def solution(mesh):
    split = Mesh(mesh.devices.reshape(mesh.shape["grp"], 16, 2, 2), GRP_EP)
    return jax.shard_map(
        shards,
        mesh=split,
        in_specs=(
            P(GRP_EP, None),
            P(GRP_EP, None),
            P(GRP_EP, None),
            P(),
            P(),
            P(EP, None, None),
            P(EP, None, None),
            P(EP, None, None),
        ),
        out_specs=P("grp", EP),
        check_vma=False,
    )
```

```python
import functools

import jax
import jax.numpy as jnp
from jax import lax
from jax.experimental import pallas as pl
from jax.experimental.pallas import tpu as pltpu
from jax.sharding import Mesh
from jax.sharding import PartitionSpec as P

EP = ("zh", "zl", "core")
CHIPS = ("zh", "zl")
GRP_EP = ("grp", "zh", "zl", "core")
LANES = 128
CLASSES = 4
CHUNKS = 4
EPSILON = 1e-06
F32 = jnp.float32
BF16 = jnp.bfloat16

VMEM = pl.BlockSpec(memory_space=pltpu.VMEM)
SMEM = pl.BlockSpec(memory_space=pltpu.SMEM)
HBM = pl.BlockSpec(memory_space=pltpu.HBM)


def by_class(parts, is_core, is_odd):
    a, b, c, d = parts
    a, b, c, d = (
        jnp.where(is_core, b, a),
        jnp.where(is_core, a, b),
        jnp.where(is_core, d, c),
        jnp.where(is_core, c, d),
    )
    return (
        jnp.where(is_odd, c, a),
        jnp.where(is_odd, d, b),
        jnp.where(is_odd, a, c),
        jnp.where(is_odd, b, d),
    )


def payload_kernel(tokens_ref, routes_ref, gates_ref, gain_ref, out_ref, meta_ref):
    width = tokens_ref.shape[1]
    per_dev = tokens_ref.shape[0]
    topk = routes_ref.shape[0]
    values = tokens_ref[...].astype(F32)
    mean = jnp.mean(values * values, axis=1, keepdims=True)
    out_ref[:, :width] = (values * lax.rsqrt(mean + EPSILON) * gain_ref[...]).astype(BF16)
    gates = gates_ref[...]
    high = gates.astype(BF16).astype(F32)
    mid = (gates - high).astype(BF16).astype(F32)
    meta_ref[...] = jnp.zeros(meta_ref.shape, F32)
    meta_ref[0:topk, 0:per_dev] = routes_ref[...].astype(F32)
    meta_ref[topk : 2 * topk, 0:per_dev] = high
    meta_ref[2 * topk : 3 * topk, 0:per_dev] = mid
    meta_ref[3 * topk : 4 * topk, 0:per_dev] = gates - high - mid
    out_ref[:, width:] = jnp.transpose(meta_ref[...])[:per_dev, :].astype(BF16)


def shed(load, capacity):
    group = load.shape[0]
    even = lax.broadcasted_iota(jnp.int32, load.shape, 0) % 2 == 0
    at = lambda x, d: pltpu.roll(x, (-d) % group, 0)
    chip = load + jnp.where(even, at(load, 1), at(load, -1))
    half = capacity // 2
    over = jnp.where(chip > capacity, jnp.maximum(load - half, 0.0), 0.0)
    kept = load - over
    settled = jnp.where(even, kept + at(kept, 1) + at(over, -2) + at(over, 3), 0.0)
    return kept, chip, settled


def windows(at_ref, keep_ref, got_ref):
    is_core = at_ref[1] == 1
    chips, cols, slots = keep_ref.shape
    keep = keep_ref[...].astype(F32).reshape(chips * cols, slots)
    got = got_ref[...].astype(F32).reshape(chips * cols, slots)
    return jnp.where(is_core, got, keep), jnp.where(is_core, keep, got)


def spill_kernel(at_ref, keep_ref, got_ref, right_ref, left_ref):
    low, high = windows(at_ref, keep_ref, got_ref)
    rows = right_ref.shape[0]
    side = LANES // 2
    lane = lax.broadcasted_iota(jnp.int32, (rows, LANES), 1)
    right_ref[...] = jnp.where(
        lane >= side, low[:rows], pltpu.roll(low[rows:], side, 1)
    ).astype(BF16)
    left_ref[...] = jnp.where(
        lane < side, high[:rows], pltpu.roll(high[rows:], side, 1)
    ).astype(BF16)


def pooled_pack_kernel(capacity, at_ref, keep_ref, got_ref, right_ref, left_ref, load_ref, out_ref, took_ref):
    low, high = windows(at_ref, keep_ref, got_ref)
    chips, cols, slots = keep_ref.shape
    extra = capacity - slots
    half = capacity // 2
    load = load_ref[...]
    group = load.shape[0]
    kept, _, _ = shed(load, capacity)
    over = load - kept
    row = lax.broadcasted_iota(jnp.int32, load.shape, 0)
    first = at_ref[0] // 2 * 2
    came = pltpu.roll(over, 2, 0) + pltpu.roll(over, group - 3, 0)
    bit = jnp.where((row % 2 == 0) & (came > 0.0), jnp.left_shift(1, row % 32 // 2), 0)
    halves = [jnp.where(row // 32 == h, bit, 0) for h in range(group // 32)]
    for h, half_bits in enumerate(halves):
        took_ref[h] = jnp.max(jnp.sum(half_bits, axis=0, keepdims=True).astype(F32)).astype(jnp.int32)
    one = lambda x, e: jnp.max(jnp.where(row == (e + group) % group, x, 0.0)).astype(jnp.int32)
    kept_low, kept_high = one(kept, first), one(kept, first + 1)
    from_left, from_right = one(over, first - 2), one(over, first + 3)
    lane = lax.broadcasted_iota(jnp.int32, low.shape, 1)
    side = LANES // 2
    unfold = lambda ref: jnp.concatenate(
        [ref[...].astype(F32), pltpu.roll(ref[...].astype(F32), side, 1)], axis=0
    )
    low = jnp.where(lane < kept_low, low, 0.0)
    high = jnp.where(lane >= slots - kept_high, high, 0.0)
    left = unfold(right_ref)
    left = jnp.where((lane >= half) & (lane < half + from_left), left, 0.0)
    right = unfold(left_ref)
    top = slots - 1 - half
    right = jnp.where((lane <= top) & (lane > top - from_right), right, 0.0)
    high = pltpu.roll(high, extra, 1)
    left = pltpu.roll(left, (kept_low - half + slots) % slots, 1)
    right = pltpu.roll(right, (capacity - 1 - kept_high - top + slots) % slots, 1)
    main = low + jnp.where(lane >= extra, high, 0.0)
    main = main + jnp.where(lane >= kept_low, left, 0.0)
    main = main + jnp.where(lane >= extra - kept_high, right, 0.0)
    tail = jnp.where(lane < extra, high, 0.0)
    tail = tail + jnp.where(lane < kept_low, left, 0.0)
    tail = tail + jnp.where(lane < extra - kept_high, right, 0.0)
    store_packed(main, tail, extra, out_ref)


def store_packed(main, tail, extra, out_ref):
    chips, packed, slots = out_ref.shape
    cols = main.shape[0] // chips
    groups = slots // extra
    each = cols // groups
    out_ref[:, :cols, :] = main.reshape(chips, cols, slots).astype(BF16)
    tail = tail.reshape(chips, cols, slots)
    out = tail[:, :each].reshape(chips * each, slots)
    for g in range(1, groups):
        out = out + pltpu.roll(
            tail[:, g * each : (g + 1) * each].reshape(chips * each, slots), g * extra, 1
        )
    out_ref[:, cols:, :] = out.reshape(chips, each, slots).astype(BF16)


def experts_kernel(
    topk, sizes, at_ref, a_ref, b_ref, c_ref, d_ref, wg_hbm, wu_hbm, wd_hbm,
    rank_ref, keep_ref, send_ref, load_ref, level_ref, wg_ref, wu_ref, wd_ref, sems,
):
    copies = []
    for i, (src, dst) in enumerate(((wg_hbm, wg_ref), (wu_hbm, wu_ref), (wd_hbm, wd_ref))):
        step = dst.shape[0] // CHUNKS
        copies.append(
            [
                pltpu.make_async_copy(
                    src.at[0, pl.ds(c * step, step)], dst.at[pl.ds(c * step, step)], sems.at[i, c]
                )
                for c in range(CHUNKS)
            ]
        )
    for copy in sum(copies, []):
        copy.start()
    width = wg_ref.shape[0]
    is_core = at_ref[1] == 1
    is_odd = at_ref[2] == 1
    me = at_ref[0].astype(F32)
    group, total = rank_ref.shape
    chips, cols, slots = keep_ref.shape
    per_dev = total // group
    part = a_ref.shape[0]
    outer = part // per_dev
    refs = (a_ref, b_ref, c_ref, d_ref)
    meta = by_class([r[:, width:].astype(F32) for r in refs], is_core, is_odd)
    grouped = jnp.concatenate([jnp.transpose(m) for m in meta], axis=1)
    rows = jnp.concatenate(
        [m[i * per_dev : (i + 1) * per_dev] for i in range(outer) for m in meta], axis=0
    )
    ordered = jnp.concatenate(
        [jnp.transpose(rows[i * LANES : (i + 1) * LANES]) for i in range(total // LANES)], axis=1
    )
    expert = lax.broadcasted_iota(jnp.int32, (group, total), 0).astype(F32)
    match = jnp.zeros((group, total), F32)
    for k in range(topk):
        match = match + jnp.where(ordered[k : k + 1, :] == expert, 1.0, 0.0)
    index = lax.broadcasted_iota(jnp.int32, (total, total), 0)
    at = lax.broadcasted_iota(jnp.int32, (total, total), 1)
    place = at % part // per_dev * (per_dev * CLASSES) + at // part * per_dev + at % per_dev
    counts = match.astype(BF16)
    rank = jnp.dot(
        counts, jnp.where(index < at, 1.0, 0.0).astype(BF16), preferred_element_type=F32
    )
    rank_ref[...] = jnp.where(match > 0.0, rank, -1.0)
    moved = jnp.dot(
        counts, jnp.where(index < place, 1.0, 0.0).astype(BF16), preferred_element_type=F32
    )
    slot = jnp.sum(jnp.where(expert == me, moved, 0.0), axis=0, keepdims=True)
    slot = jnp.where(is_core, slots - 1 - slot, slot)
    gates = grouped[topk : 2 * topk] + grouped[2 * topk : 3 * topk] + grouped[3 * topk : 4 * topk]
    mine = jnp.zeros((1, total), F32)
    gate = jnp.zeros((1, total), F32)
    for k in range(topk):
        named = grouped[k : k + 1, :] == me
        mine = jnp.where(named, 1.0, mine)
        gate = jnp.where(named, gates[k : k + 1, :], gate)
    slot = jnp.where(mine > 0.0, slot, -1.0).astype(jnp.int32)
    gate = jnp.concatenate(
        by_class([gate[:, k * part : (k + 1) * part] for k in range(CLASSES)], is_core, is_odd), axis=1
    )
    slot = jnp.concatenate(
        by_class([slot[:, k * part : (k + 1) * part] for k in range(CLASSES)], is_core, is_odd), axis=1
    )
    load = jnp.broadcast_to(jnp.sum(match, axis=1, keepdims=True), (group, LANES))
    load_ref[...] = load
    kept, chip, settled = shed(load, sizes[0])
    most = jnp.max(chip).astype(jnp.int32)
    fits = (jnp.max(settled).astype(jnp.int32) <= sizes[0]).astype(jnp.int32)
    level_ref[0] = jnp.where(
        most <= sizes[0], 0, jnp.where(most <= sizes[1], 1, 3 - fits)
    ).astype(jnp.int32)

    hit = lax.broadcasted_iota(jnp.int32, (slots, total), 0) == slot
    pick = jnp.where(hit, 1.0, 0.0).astype(BF16)
    gate = jnp.sum(jnp.where(hit, gate, 0.0), axis=1, keepdims=True)
    picked = jnp.zeros((slots, width), F32)
    for k, ref in enumerate(refs):
        picked = picked + jnp.dot(
            pick[:, k * part : (k + 1) * part], ref[:, :width], preferred_element_type=F32
        )
    picked = picked.astype(BF16)
    for copy in copies[0]:
        copy.wait()
    gate_val = jnp.dot(picked, wg_ref[...], preferred_element_type=F32)
    for copy in copies[1]:
        copy.wait()
    up_val = jnp.dot(picked, wu_ref[...], preferred_element_type=F32)
    act = (gate_val * jax.nn.sigmoid(gate_val) * up_val * gate).astype(BF16)
    for copy in copies[2]:
        copy.wait()
    result = jnp.dot(act, wd_ref[...], preferred_element_type=F32)
    result = jnp.transpose(result).reshape(chips, 2, cols, slots)
    even, odd = result[:, 0], result[:, 1]
    keep_ref[...] = jnp.where(is_core, odd, even).astype(BF16)
    send_ref[...] = jnp.where(is_core, even, odd).astype(BF16)


def pack_kernel(capacity, at_ref, keep_ref, got_ref, out_ref):
    low, high = windows(at_ref, keep_ref, got_ref)
    extra = capacity - keep_ref.shape[2]
    if extra == keep_ref.shape[2]:
        main, tail = low, high
    else:
        high = pltpu.roll(high, extra, 1)
        spill = lax.broadcasted_iota(jnp.int32, high.shape, 1) < extra
        main = low + jnp.where(spill, 0.0, high)
        tail = jnp.where(spill, high, 0.0)
    store_packed(main, tail, extra, out_ref)


def combine_kernel(capacity, pooled, took_ref, rows_ref, rank_ref, load_ref, out_ref, square_ref, kept_ref):
    cols, total = out_ref.shape
    chips = rows_ref.shape[0]
    extra = capacity - LANES
    groups = LANES // extra
    each = cols // groups
    slot = lax.broadcasted_iota(jnp.int32, (capacity, total), 0).astype(F32).astype(BF16)
    col = lax.broadcasted_iota(jnp.int32, (cols, LANES), 0)
    lane = lax.broadcasted_iota(jnp.int32, (cols, LANES), 1)
    own = (col // each) == (lane // extra)
    one = jnp.ones((), BF16)
    zero = jnp.zeros((), BF16)
    group = rank_ref.shape[0]
    half = capacity // 2
    if pooled:
        kept, _, _ = shed(load_ref[...], capacity)
        kept_ref[...] = jnp.concatenate([kept] * (total // LANES), axis=1)

    def add(s, acc, hit):
        pick = jnp.where(hit, one, zero)
        pick = jnp.concatenate([pick[:LANES]] + [pick[LANES:]] * groups, axis=0)
        block = rows_ref[s].astype(F32)
        tail = jnp.concatenate([block[cols:]] * groups, axis=0)
        tail = jnp.where(own, tail, 0.0)
        left = jnp.concatenate([block[:cols], tail], axis=1).astype(BF16)
        return acc + jnp.dot(left, pick, preferred_element_type=F32)

    def keys(s):
        low = rank_ref[pl.ds(2 * s, 1), :]
        high = rank_ref[pl.ds(2 * s + 1, 1), :]
        if pooled:
            low = jnp.where(low < kept_ref[pl.ds(2 * s, 1), :], low, -1.0)
            high = jnp.where(high < kept_ref[pl.ds(2 * s + 1, 1), :], high, -1.0)
        high = jnp.where(high < 0.0, -1.0, capacity - 1.0 - high)
        return (slot == low.astype(BF16)) | (slot == high.astype(BF16))

    def step(s, acc):
        return add(s, acc, keys(s))

    out = lax.fori_loop(0, chips, step, jnp.zeros((cols, total), F32), unroll=8)
    if pooled:

        def more(s, acc):
            def surplus(acc):
                before = lax.rem(2 * s - 2 + group, group)
                after = lax.rem(2 * s + 3, group)
                left = rank_ref[pl.ds(before, 1), :]
                right = rank_ref[pl.ds(after, 1), :]
                left = jnp.where(
                    left < kept_ref[pl.ds(before, 1), :],
                    -1.0,
                    kept_ref[pl.ds(2 * s, 1), :] + left - half,
                )
                right = jnp.where(
                    right < kept_ref[pl.ds(after, 1), :],
                    -1.0,
                    capacity - 1.0 - (kept_ref[pl.ds(2 * s + 1, 1), :] + right - half),
                )
                return add(s, acc, (slot == left.astype(BF16)) | (slot == right.astype(BF16)))

            took = (took_ref[s // 16] >> (s % 16)) & 1
            return lax.cond(took == 1, surplus, lambda acc: acc, acc)

        out = lax.fori_loop(0, chips, more, out)
    out_ref[...] = out
    square_ref[...] = jnp.sum(out * out, axis=0, keepdims=True)


def spread_kernel(mine_ref, other_ref, out_ref):
    square = mine_ref[...] + other_ref[...]
    chips, lines, _ = out_ref.shape
    for i in range(lines):
        out_ref[:, i : i + 1, :] = jnp.broadcast_to(
            square[None, :, i * LANES : (i + 1) * LANES], (chips, 1, LANES)
        ).astype(BF16)


def finish_kernel(width, at_ref, squares_ref, mixed_ref, gain_ref, out_ref):
    sums = jnp.sum(squares_ref[...].astype(F32), axis=0)
    mean = jnp.concatenate([sums[i : i + 1] for i in range(sums.shape[0])], axis=1) / width
    cols = mixed_ref.shape[0]
    each = LANES // cols
    me = at_ref[0]
    gain = jnp.broadcast_to(gain_ref[pl.ds(me // each, 1), :], (LANES, LANES))
    gain = pltpu.roll(gain, (each - me % each) % each * cols, 1)
    gain = jnp.transpose(gain)[:cols, :1]
    out_ref[...] = (mixed_ref[...] * lax.rsqrt(mean + EPSILON) * gain).astype(BF16)


def shards(tokens, routes, gate_weights, norm_gain, final_gain, w_gate, w_up, w_down):
    per_dev, width = tokens.shape
    topk = routes.shape[1]
    group = lax.axis_size(EP)
    chips = group // 2
    cols = width // group
    total = per_dev * group
    most = 2 * group
    me = lax.axis_index(EP)
    core = lax.axis_index("core")
    odd = lax.axis_index("zl")
    at = jnp.stack([me, core, odd]).astype(jnp.int32)

    payload = pl.pallas_call(
        payload_kernel,
        out_shape=jax.ShapeDtypeStruct((per_dev, width + LANES), BF16),
        scratch_shapes=[pltpu.VMEM((LANES, LANES), F32)],
    )(tokens, jnp.transpose(routes), jnp.transpose(gate_weights), norm_gain[None, :])

    zigzag = []
    for chip in range(chips):
        zigzag.append((chip * 2, ((chip + 1) % chips) * 2))
        zigzag.append((chip * 2 + 1, ((chip - 1) % chips) * 2 + 1))
    swap = [(0, 1), (1, 0)]
    own = lax.all_gather(payload, "zh", axis=0, tiled=True)
    near = lax.ppermute(own, EP, zigzag)
    own_pair = lax.ppermute(own, "core", swap)
    near_pair = lax.ppermute(near, "core", swap)
    pieces = (own, own_pair, near, near_pair)
    part = own.shape[0]

    window = jax.ShapeDtypeStruct((chips, cols, LANES), BF16)
    sizes = (most * 5 // 4, most * 3 // 2, most * 2)
    rank, keep, send, load, level = pl.pallas_call(
        functools.partial(experts_kernel, topk, sizes),
        in_specs=[SMEM] + [VMEM] * CLASSES + [HBM] * 3,
        out_specs=[VMEM, VMEM, VMEM, VMEM, SMEM],
        out_shape=[
            jax.ShapeDtypeStruct((group, total), F32),
            window,
            window,
            jax.ShapeDtypeStruct((group, LANES), F32),
            jax.ShapeDtypeStruct((1,), jnp.int32),
        ],
        scratch_shapes=[
            pltpu.VMEM(w_gate.shape[1:], BF16),
            pltpu.VMEM(w_up.shape[1:], BF16),
            pltpu.VMEM(w_down.shape[1:], BF16),
            pltpu.SemaphoreType.DMA((3, CHUNKS)),
        ],
        compiler_params=pltpu.CompilerParams(vmem_limit_bytes=50 << 20),
    )(at, *pieces, w_gate, w_up, w_down)
    got = lax.ppermute(send, "core", swap)
    lines = total // LANES

    right = [(i, (i + 2) % group) for i in range(group)]
    left = [(i, (i - 2) % group) for i in range(group)]
    small = pltpu.CompilerParams(vmem_limit_bytes=16 << 20)

    def branch(capacity, pooled):
        packed = cols * capacity // LANES
        message = jax.ShapeDtypeStruct((chips, packed, LANES), BF16)
        spill = jax.ShapeDtypeStruct((chips * cols // 2, LANES), BF16)

        def run(at, keep, got, rank, load):
            if pooled:
                to_right, to_left = pl.pallas_call(
                    spill_kernel,
                    in_specs=[SMEM, VMEM, VMEM],
                    out_shape=[spill, spill],
                    compiler_params=small,
                )(at, keep, got)
                both, took = pl.pallas_call(
                    functools.partial(pooled_pack_kernel, capacity),
                    in_specs=[SMEM] + [VMEM] * 5,
                    out_specs=[VMEM, SMEM],
                    out_shape=[message, jax.ShapeDtypeStruct((group // 32,), jnp.int32)],
                    compiler_params=small,
                )(at, keep, got, lax.ppermute(to_right, EP, right), lax.ppermute(to_left, EP, left), load)
            else:
                took = at
                both = pl.pallas_call(
                    functools.partial(pack_kernel, capacity),
                    in_specs=[SMEM, VMEM, VMEM],
                    out_shape=message,
                    compiler_params=small,
                )(at, keep, got)
            returned = lax.all_to_all(both, CHIPS, split_axis=0, concat_axis=0, tiled=True)
            return pl.pallas_call(
                functools.partial(combine_kernel, capacity, pooled),
                in_specs=[SMEM] + [VMEM] * 3,
                out_shape=[
                    jax.ShapeDtypeStruct((cols, total), F32),
                    jax.ShapeDtypeStruct((1, total), F32),
                ],
                scratch_shapes=[pltpu.VMEM((group, total), F32)],
                compiler_params=small,
            )(took, returned, rank, load)

        return run

    mixed, square = lax.switch(
        level[0],
        [branch(sizes[0], False), branch(sizes[1], False), branch(sizes[0], True), branch(sizes[2], False)],
        at, keep, got, rank, load,
    )

    spread = pl.pallas_call(
        spread_kernel,
        in_specs=[VMEM] * 2,
        out_shape=jax.ShapeDtypeStruct((chips, total // LANES, LANES), BF16),
        compiler_params=small,
    )(square, lax.ppermute(square, "core", swap))
    squares = lax.all_to_all(spread, CHIPS, split_axis=0, concat_axis=0, tiled=True)
    finished = pl.pallas_call(
        functools.partial(finish_kernel, width),
        in_specs=[SMEM] + [VMEM] * 3,
        out_shape=jax.ShapeDtypeStruct((cols, total), BF16),
        compiler_params=small,
    )(at, squares, mixed, final_gain.reshape(-1, LANES))
    return jnp.transpose(finished)


def solution(mesh):
    split = Mesh(mesh.devices.reshape(mesh.shape["grp"], 16, 2, 2), GRP_EP)
    return jax.shard_map(
        shards,
        mesh=split,
        in_specs=(
            P(GRP_EP, None),
            P(GRP_EP, None),
            P(GRP_EP, None),
            P(),
            P(),
            P(EP, None, None),
            P(EP, None, None),
            P(EP, None, None),
        ),
        out_specs=P("grp", EP),
        check_vma=False,
    )
```

```python
import functools

import jax
import jax.numpy as jnp
from jax import lax
from jax.experimental import pallas as pl
from jax.experimental.pallas import tpu as pltpu
from jax.sharding import Mesh
from jax.sharding import PartitionSpec as P

EP = ("zh", "zl", "core")
CHIPS = ("zh", "zl")
GRP_EP = ("grp", "zh", "zl", "core")
LANES = 128
CLASSES = 4
CHUNKS = 4
BATCH = 8
EPSILON = 1e-06
F32 = jnp.float32
BF16 = jnp.bfloat16

VMEM = pl.BlockSpec(memory_space=pltpu.VMEM)
SMEM = pl.BlockSpec(memory_space=pltpu.SMEM)
HBM = pl.BlockSpec(memory_space=pltpu.HBM)


def by_class(parts, is_core, is_odd):
    a, b, c, d = parts
    a, b, c, d = (
        jnp.where(is_core, b, a),
        jnp.where(is_core, a, b),
        jnp.where(is_core, d, c),
        jnp.where(is_core, c, d),
    )
    return (
        jnp.where(is_odd, c, a),
        jnp.where(is_odd, d, b),
        jnp.where(is_odd, a, c),
        jnp.where(is_odd, b, d),
    )


def payload_kernel(tokens_ref, routes_ref, gates_ref, gain_ref, out_ref, meta_ref):
    width = tokens_ref.shape[1]
    per_dev = tokens_ref.shape[0]
    topk = routes_ref.shape[0]
    values = tokens_ref[...].astype(F32)
    mean = jnp.mean(values * values, axis=1, keepdims=True)
    out_ref[:, :width] = (values * lax.rsqrt(mean + EPSILON) * gain_ref[...]).astype(BF16)
    gates = gates_ref[...]
    high = gates.astype(BF16).astype(F32)
    mid = (gates - high).astype(BF16).astype(F32)
    meta_ref[...] = jnp.zeros(meta_ref.shape, F32)
    meta_ref[0:topk, 0:per_dev] = routes_ref[...].astype(F32)
    meta_ref[topk : 2 * topk, 0:per_dev] = high
    meta_ref[2 * topk : 3 * topk, 0:per_dev] = mid
    meta_ref[3 * topk : 4 * topk, 0:per_dev] = gates - high - mid
    out_ref[:, width:] = jnp.transpose(meta_ref[...])[:per_dev, :].astype(BF16)


def shed(load, capacity):
    group = load.shape[0]
    even = lax.broadcasted_iota(jnp.int32, load.shape, 0) % 2 == 0
    at = lambda x, d: pltpu.roll(x, (-d) % group, 0)
    chip = load + jnp.where(even, at(load, 1), at(load, -1))
    half = capacity // 2
    over = jnp.where(chip > capacity, jnp.maximum(load - half, 0.0), 0.0)
    kept = load - over
    settled = jnp.where(even, kept + at(kept, 1) + at(over, -2) + at(over, 3), 0.0)
    return kept, chip, settled


def windows(at_ref, keep_ref, got_ref):
    is_core = at_ref[1] == 1
    chips, cols, slots = keep_ref.shape
    keep = keep_ref[...].astype(F32).reshape(chips * cols, slots)
    got = got_ref[...].astype(F32).reshape(chips * cols, slots)
    return jnp.where(is_core, got, keep), jnp.where(is_core, keep, got)


def spill_kernel(at_ref, keep_ref, got_ref, right_ref, left_ref):
    low, high = windows(at_ref, keep_ref, got_ref)
    rows = right_ref.shape[0]
    side = LANES // 2
    lane = lax.broadcasted_iota(jnp.int32, (rows, LANES), 1)
    right_ref[...] = jnp.where(
        lane >= side, low[:rows], pltpu.roll(low[rows:], side, 1)
    ).astype(BF16)
    left_ref[...] = jnp.where(
        lane < side, high[:rows], pltpu.roll(high[rows:], side, 1)
    ).astype(BF16)


def pooled_pack_kernel(capacity, at_ref, keep_ref, got_ref, right_ref, left_ref, load_ref, out_ref, took_ref):
    low, high = windows(at_ref, keep_ref, got_ref)
    chips, cols, slots = keep_ref.shape
    extra = capacity - slots
    half = capacity // 2
    load = load_ref[...]
    group = load.shape[0]
    kept, _, _ = shed(load, capacity)
    over = load - kept
    row = lax.broadcasted_iota(jnp.int32, load.shape, 0)
    first = at_ref[0] // 2 * 2
    came = pltpu.roll(over, 2, 0) + pltpu.roll(over, group - 3, 0)
    bit = jnp.where((row % 2 == 0) & (came > 0.0), jnp.left_shift(1, row % 32 // 2), 0)
    halves = [jnp.where(row // 32 == h, bit, 0) for h in range(group // 32)]
    for h, half_bits in enumerate(halves):
        took_ref[h] = jnp.max(jnp.sum(half_bits, axis=0, keepdims=True).astype(F32)).astype(jnp.int32)
    one = lambda x, e: jnp.max(jnp.where(row == (e + group) % group, x, 0.0)).astype(jnp.int32)
    kept_low, kept_high = one(kept, first), one(kept, first + 1)
    from_left, from_right = one(over, first - 2), one(over, first + 3)
    lane = lax.broadcasted_iota(jnp.int32, low.shape, 1)
    side = LANES // 2
    unfold = lambda ref: jnp.concatenate(
        [ref[...].astype(F32), pltpu.roll(ref[...].astype(F32), side, 1)], axis=0
    )
    low = jnp.where(lane < kept_low, low, 0.0)
    high = jnp.where(lane >= slots - kept_high, high, 0.0)
    left = unfold(right_ref)
    left = jnp.where((lane >= half) & (lane < half + from_left), left, 0.0)
    right = unfold(left_ref)
    top = slots - 1 - half
    right = jnp.where((lane <= top) & (lane > top - from_right), right, 0.0)
    high = pltpu.roll(high, extra, 1)
    left = pltpu.roll(left, (kept_low - half + slots) % slots, 1)
    right = pltpu.roll(right, (capacity - 1 - kept_high - top + slots) % slots, 1)
    main = low + jnp.where(lane >= extra, high, 0.0)
    main = main + jnp.where(lane >= kept_low, left, 0.0)
    main = main + jnp.where(lane >= extra - kept_high, right, 0.0)
    tail = jnp.where(lane < extra, high, 0.0)
    tail = tail + jnp.where(lane < kept_low, left, 0.0)
    tail = tail + jnp.where(lane < extra - kept_high, right, 0.0)
    store_packed(main, tail, extra, out_ref)


def store_packed(main, tail, extra, out_ref):
    chips, packed, slots = out_ref.shape
    cols = main.shape[0] // chips
    groups = slots // extra
    each = cols // groups
    out_ref[:, :cols, :] = main.reshape(chips, cols, slots).astype(BF16)
    tail = tail.reshape(chips, cols, slots)
    out = tail[:, :each].reshape(chips * each, slots)
    for g in range(1, groups):
        out = out + pltpu.roll(
            tail[:, g * each : (g + 1) * each].reshape(chips * each, slots), g * extra, 1
        )
    out_ref[:, cols:, :] = out.reshape(chips, each, slots).astype(BF16)


def experts_kernel(
    topk, sizes, at_ref, a_ref, b_ref, c_ref, d_ref, wg_hbm, wu_hbm, wd_hbm,
    rank_ref, keep_ref, send_ref, load_ref, level_ref, wg_ref, wu_ref, wd_ref, sems,
):
    copies = []
    for i, (src, dst) in enumerate(((wg_hbm, wg_ref), (wu_hbm, wu_ref), (wd_hbm, wd_ref))):
        step = dst.shape[0] // CHUNKS
        copies.append(
            [
                pltpu.make_async_copy(
                    src.at[0, pl.ds(c * step, step)], dst.at[pl.ds(c * step, step)], sems.at[i, c]
                )
                for c in range(CHUNKS)
            ]
        )
    for copy in sum(copies, []):
        copy.start()
    width = wg_ref.shape[0]
    is_core = at_ref[1] == 1
    is_odd = at_ref[2] == 1
    me = at_ref[0].astype(F32)
    group, total = rank_ref.shape
    chips, cols, slots = keep_ref.shape
    per_dev = total // group
    part = a_ref.shape[0]
    outer = part // per_dev
    refs = (a_ref, b_ref, c_ref, d_ref)
    meta = by_class([r[:, width:].astype(F32) for r in refs], is_core, is_odd)
    grouped = jnp.concatenate([jnp.transpose(m) for m in meta], axis=1)
    rows = jnp.concatenate(
        [m[i * per_dev : (i + 1) * per_dev] for i in range(outer) for m in meta], axis=0
    )
    ordered = jnp.concatenate(
        [jnp.transpose(rows[i * LANES : (i + 1) * LANES]) for i in range(total // LANES)], axis=1
    )
    expert = lax.broadcasted_iota(jnp.int32, (group, total), 0).astype(F32)
    match = jnp.zeros((group, total), F32)
    for k in range(topk):
        match = match + jnp.where(ordered[k : k + 1, :] == expert, 1.0, 0.0)
    index = lax.broadcasted_iota(jnp.int32, (total, total), 0)
    at = lax.broadcasted_iota(jnp.int32, (total, total), 1)
    place = at % part // per_dev * (per_dev * CLASSES) + at // part * per_dev + at % per_dev
    counts = match.astype(BF16)
    rank = jnp.dot(
        counts, jnp.where(index < at, 1.0, 0.0).astype(BF16), preferred_element_type=F32
    )
    rank_ref[...] = jnp.where(match > 0.0, rank, -1.0)
    moved = jnp.dot(
        counts, jnp.where(index < place, 1.0, 0.0).astype(BF16), preferred_element_type=F32
    )
    slot = jnp.sum(jnp.where(expert == me, moved, 0.0), axis=0, keepdims=True)
    slot = jnp.where(is_core, slots - 1 - slot, slot)
    gates = grouped[topk : 2 * topk] + grouped[2 * topk : 3 * topk] + grouped[3 * topk : 4 * topk]
    mine = jnp.zeros((1, total), F32)
    gate = jnp.zeros((1, total), F32)
    for k in range(topk):
        named = grouped[k : k + 1, :] == me
        mine = jnp.where(named, 1.0, mine)
        gate = jnp.where(named, gates[k : k + 1, :], gate)
    slot = jnp.where(mine > 0.0, slot, -1.0).astype(jnp.int32)
    gate = jnp.concatenate(
        by_class([gate[:, k * part : (k + 1) * part] for k in range(CLASSES)], is_core, is_odd), axis=1
    )
    slot = jnp.concatenate(
        by_class([slot[:, k * part : (k + 1) * part] for k in range(CLASSES)], is_core, is_odd), axis=1
    )
    load = jnp.broadcast_to(jnp.sum(match, axis=1, keepdims=True), (group, LANES))
    load_ref[...] = load
    kept, chip, settled = shed(load, sizes[0])
    most = jnp.max(chip).astype(jnp.int32)
    fits = (jnp.max(settled).astype(jnp.int32) <= sizes[0]).astype(jnp.int32)
    level_ref[0] = jnp.where(
        most <= sizes[0], 0, jnp.where(most <= sizes[1], 1, 3 - fits)
    ).astype(jnp.int32)

    hit = lax.broadcasted_iota(jnp.int32, (slots, total), 0) == slot
    pick = jnp.where(hit, 1.0, 0.0).astype(BF16)
    gate = jnp.sum(jnp.where(hit, gate, 0.0), axis=1, keepdims=True)
    picked = jnp.zeros((slots, width), F32)
    for k, ref in enumerate(refs):
        picked = picked + jnp.dot(
            pick[:, k * part : (k + 1) * part], ref[:, :width], preferred_element_type=F32
        )
    picked = picked.astype(BF16)
    for copy in copies[0]:
        copy.wait()
    gate_val = jnp.dot(picked, wg_ref[...], preferred_element_type=F32)
    for copy in copies[1]:
        copy.wait()
    up_val = jnp.dot(picked, wu_ref[...], preferred_element_type=F32)
    act = (gate_val * jax.nn.sigmoid(gate_val) * up_val * gate).astype(BF16)
    for copy in copies[2]:
        copy.wait()
    result = jnp.dot(act, wd_ref[...], preferred_element_type=F32)
    result = jnp.transpose(result).reshape(chips, 2, cols, slots)
    even, odd = result[:, 0], result[:, 1]
    keep_ref[...] = jnp.where(is_core, odd, even).astype(BF16)
    send_ref[...] = jnp.where(is_core, even, odd).astype(BF16)


def pack_kernel(capacity, at_ref, keep_ref, got_ref, out_ref):
    low, high = windows(at_ref, keep_ref, got_ref)
    extra = capacity - keep_ref.shape[2]
    if extra == keep_ref.shape[2]:
        main, tail = low, high
    else:
        high = pltpu.roll(high, extra, 1)
        spill = lax.broadcasted_iota(jnp.int32, high.shape, 1) < extra
        main = low + jnp.where(spill, 0.0, high)
        tail = jnp.where(spill, high, 0.0)
    store_packed(main, tail, extra, out_ref)


def combine_kernel(capacity, pooled, took_ref, rows_ref, rank_ref, load_ref, out_ref, square_ref, kept_ref):
    cols, total = out_ref.shape
    chips = rows_ref.shape[0]
    extra = capacity - LANES
    groups = LANES // extra
    each = cols // groups
    slot = lax.broadcasted_iota(jnp.int32, (capacity, total), 0).astype(F32).astype(BF16)
    col = lax.broadcasted_iota(jnp.int32, (cols, LANES), 0)
    lane = lax.broadcasted_iota(jnp.int32, (cols, LANES), 1)
    own = (col // each) == (lane // extra)
    one = jnp.ones((), BF16)
    zero = jnp.zeros((), BF16)
    group = rank_ref.shape[0]
    half = capacity // 2
    if pooled:
        kept, _, _ = shed(load_ref[...], capacity)
        kept_ref[...] = jnp.concatenate([kept] * (total // LANES), axis=1)

    def add(s, acc, hit):
        pick = jnp.where(hit, one, zero)
        pick = jnp.concatenate([pick[:LANES]] + [pick[LANES:]] * groups, axis=0)
        block = rows_ref[s].astype(F32)
        tail = jnp.concatenate([block[cols:]] * groups, axis=0)
        tail = jnp.where(own, tail, 0.0)
        left = jnp.concatenate([block[:cols], tail], axis=1).astype(BF16)
        return acc + jnp.dot(left, pick, preferred_element_type=F32)

    def keys(s):
        low = rank_ref[pl.ds(2 * s, 1), :]
        high = rank_ref[pl.ds(2 * s + 1, 1), :]
        if pooled:
            low = jnp.where(low < kept_ref[pl.ds(2 * s, 1), :], low, -1.0)
            high = jnp.where(high < kept_ref[pl.ds(2 * s + 1, 1), :], high, -1.0)
        high = jnp.where(high < 0.0, -1.0, capacity - 1.0 - high)
        return (slot == low.astype(BF16)) | (slot == high.astype(BF16))

    def step(i, acc):
        mains, tails, main_picks, tail_picks = [], [], [], []
        for first in range(0, BATCH, groups):
            spread = jnp.zeros((cols, LANES), F32)
            for q in range(groups):
                s = i * BATCH + first + q
                pick = jnp.where(keys(s), one, zero)
                main_picks.append(pick[:LANES])
                tail_picks.append(pick[LANES:])
                block = rows_ref[s].astype(F32)
                mains.append(block[:cols])
                tail = block[cols:]
                turned = [tail] + [pltpu.roll(tail, k * extra, 1) for k in range(1, groups)]
                tail = jnp.concatenate([turned[(q - g) % groups] for g in range(groups)], axis=0)
                spread = jnp.where(lane // extra == q, tail, spread)
            tails.append(spread)
        left = jnp.concatenate(mains + tails, axis=1).astype(BF16)
        pick = jnp.concatenate(main_picks + tail_picks, axis=0)
        return acc + jnp.dot(left, pick, preferred_element_type=F32)

    out = lax.fori_loop(0, chips // BATCH, step, jnp.zeros((cols, total), F32), unroll=2)
    if pooled:

        def more(s, acc):
            def surplus(acc):
                before = lax.rem(2 * s - 2 + group, group)
                after = lax.rem(2 * s + 3, group)
                left = rank_ref[pl.ds(before, 1), :]
                right = rank_ref[pl.ds(after, 1), :]
                left = jnp.where(
                    left < kept_ref[pl.ds(before, 1), :],
                    -1.0,
                    kept_ref[pl.ds(2 * s, 1), :] + left - half,
                )
                right = jnp.where(
                    right < kept_ref[pl.ds(after, 1), :],
                    -1.0,
                    capacity - 1.0 - (kept_ref[pl.ds(2 * s + 1, 1), :] + right - half),
                )
                return add(s, acc, (slot == left.astype(BF16)) | (slot == right.astype(BF16)))

            took = (took_ref[s // 16] >> (s % 16)) & 1
            return lax.cond(took == 1, surplus, lambda acc: acc, acc)

        out = lax.fori_loop(0, chips, more, out)
    out_ref[...] = out
    square_ref[...] = jnp.sum(out * out, axis=0, keepdims=True)


def spread_kernel(mine_ref, other_ref, out_ref):
    square = mine_ref[...] + other_ref[...]
    chips, lines, _ = out_ref.shape
    for i in range(lines):
        out_ref[:, i : i + 1, :] = jnp.broadcast_to(
            square[None, :, i * LANES : (i + 1) * LANES], (chips, 1, LANES)
        ).astype(BF16)


def finish_kernel(width, at_ref, squares_ref, mixed_ref, gain_ref, out_ref):
    sums = jnp.sum(squares_ref[...].astype(F32), axis=0)
    mean = jnp.concatenate([sums[i : i + 1] for i in range(sums.shape[0])], axis=1) / width
    cols = mixed_ref.shape[0]
    each = LANES // cols
    me = at_ref[0]
    gain = jnp.broadcast_to(gain_ref[pl.ds(me // each, 1), :], (LANES, LANES))
    gain = pltpu.roll(gain, (each - me % each) % each * cols, 1)
    gain = jnp.transpose(gain)[:cols, :1]
    out_ref[...] = (mixed_ref[...] * lax.rsqrt(mean + EPSILON) * gain).astype(BF16)


def shards(tokens, routes, gate_weights, norm_gain, final_gain, w_gate, w_up, w_down):
    per_dev, width = tokens.shape
    topk = routes.shape[1]
    group = lax.axis_size(EP)
    chips = group // 2
    cols = width // group
    total = per_dev * group
    most = 2 * group
    me = lax.axis_index(EP)
    core = lax.axis_index("core")
    odd = lax.axis_index("zl")
    at = jnp.stack([me, core, odd]).astype(jnp.int32)

    payload = pl.pallas_call(
        payload_kernel,
        out_shape=jax.ShapeDtypeStruct((per_dev, width + LANES), BF16),
        scratch_shapes=[pltpu.VMEM((LANES, LANES), F32)],
    )(tokens, jnp.transpose(routes), jnp.transpose(gate_weights), norm_gain[None, :])

    zigzag = []
    for chip in range(chips):
        zigzag.append((chip * 2, ((chip + 1) % chips) * 2))
        zigzag.append((chip * 2 + 1, ((chip - 1) % chips) * 2 + 1))
    swap = [(0, 1), (1, 0)]
    own = lax.all_gather(payload, "zh", axis=0, tiled=True)
    near = lax.ppermute(own, EP, zigzag)
    own_pair = lax.ppermute(own, "core", swap)
    near_pair = lax.ppermute(near, "core", swap)
    pieces = (own, own_pair, near, near_pair)
    part = own.shape[0]

    window = jax.ShapeDtypeStruct((chips, cols, LANES), BF16)
    sizes = (most * 5 // 4, most * 3 // 2, most * 2)
    rank, keep, send, load, level = pl.pallas_call(
        functools.partial(experts_kernel, topk, sizes),
        in_specs=[SMEM] + [VMEM] * CLASSES + [HBM] * 3,
        out_specs=[VMEM, VMEM, VMEM, VMEM, SMEM],
        out_shape=[
            jax.ShapeDtypeStruct((group, total), F32),
            window,
            window,
            jax.ShapeDtypeStruct((group, LANES), F32),
            jax.ShapeDtypeStruct((1,), jnp.int32),
        ],
        scratch_shapes=[
            pltpu.VMEM(w_gate.shape[1:], BF16),
            pltpu.VMEM(w_up.shape[1:], BF16),
            pltpu.VMEM(w_down.shape[1:], BF16),
            pltpu.SemaphoreType.DMA((3, CHUNKS)),
        ],
        compiler_params=pltpu.CompilerParams(vmem_limit_bytes=50 << 20),
    )(at, *pieces, w_gate, w_up, w_down)
    got = lax.ppermute(send, "core", swap)
    lines = total // LANES

    right = [(i, (i + 2) % group) for i in range(group)]
    left = [(i, (i - 2) % group) for i in range(group)]
    small = pltpu.CompilerParams(vmem_limit_bytes=16 << 20)

    def branch(capacity, pooled):
        packed = cols * capacity // LANES
        message = jax.ShapeDtypeStruct((chips, packed, LANES), BF16)
        spill = jax.ShapeDtypeStruct((chips * cols // 2, LANES), BF16)

        def run(at, keep, got, rank, load):
            if pooled:
                to_right, to_left = pl.pallas_call(
                    spill_kernel,
                    in_specs=[SMEM, VMEM, VMEM],
                    out_shape=[spill, spill],
                    compiler_params=small,
                )(at, keep, got)
                both, took = pl.pallas_call(
                    functools.partial(pooled_pack_kernel, capacity),
                    in_specs=[SMEM] + [VMEM] * 5,
                    out_specs=[VMEM, SMEM],
                    out_shape=[message, jax.ShapeDtypeStruct((group // 32,), jnp.int32)],
                    compiler_params=small,
                )(at, keep, got, lax.ppermute(to_right, EP, right), lax.ppermute(to_left, EP, left), load)
            else:
                took = at
                both = pl.pallas_call(
                    functools.partial(pack_kernel, capacity),
                    in_specs=[SMEM, VMEM, VMEM],
                    out_shape=message,
                    compiler_params=small,
                )(at, keep, got)
            returned = lax.all_to_all(both, CHIPS, split_axis=0, concat_axis=0, tiled=True)
            return pl.pallas_call(
                functools.partial(combine_kernel, capacity, pooled),
                in_specs=[SMEM] + [VMEM] * 3,
                out_shape=[
                    jax.ShapeDtypeStruct((cols, total), F32),
                    jax.ShapeDtypeStruct((1, total), F32),
                ],
                scratch_shapes=[pltpu.VMEM((group, total), F32)],
                compiler_params=small,
            )(took, returned, rank, load)

        return run

    mixed, square = lax.switch(
        level[0],
        [branch(sizes[0], False), branch(sizes[1], False), branch(sizes[0], True), branch(sizes[2], False)],
        at, keep, got, rank, load,
    )

    spread = pl.pallas_call(
        spread_kernel,
        in_specs=[VMEM] * 2,
        out_shape=jax.ShapeDtypeStruct((chips, total // LANES, LANES), BF16),
        compiler_params=small,
    )(square, lax.ppermute(square, "core", swap))
    squares = lax.all_to_all(spread, CHIPS, split_axis=0, concat_axis=0, tiled=True)
    finished = pl.pallas_call(
        functools.partial(finish_kernel, width),
        in_specs=[SMEM] + [VMEM] * 3,
        out_shape=jax.ShapeDtypeStruct((cols, total), BF16),
        compiler_params=small,
    )(at, squares, mixed, final_gain.reshape(-1, LANES))
    return jnp.transpose(finished)


def solution(mesh):
    split = Mesh(mesh.devices.reshape(mesh.shape["grp"], 16, 2, 2), GRP_EP)
    return jax.shard_map(
        shards,
        mesh=split,
        in_specs=(
            P(GRP_EP, None),
            P(GRP_EP, None),
            P(GRP_EP, None),
            P(),
            P(),
            P(EP, None, None),
            P(EP, None, None),
            P(EP, None, None),
        ),
        out_specs=P("grp", EP),
        check_vma=False,
    )
```

```python
import functools

import jax
import jax.numpy as jnp
from jax import lax
from jax.experimental import pallas as pl
from jax.experimental.pallas import tpu as pltpu
from jax.sharding import Mesh
from jax.sharding import PartitionSpec as P

EP = ("zh", "zl", "core")
CHIPS = ("zh", "zl")
GRP_EP = ("grp", "zh", "zl", "core")
LANES = 128
CLASSES = 4
CHUNKS = 4
BATCH = 8
EPSILON = 1e-06
F32 = jnp.float32
BF16 = jnp.bfloat16

VMEM = pl.BlockSpec(memory_space=pltpu.VMEM)
SMEM = pl.BlockSpec(memory_space=pltpu.SMEM)
HBM = pl.BlockSpec(memory_space=pltpu.HBM)


def by_class(parts, is_core, is_odd):
    a, b, c, d = parts
    a, b, c, d = (
        jnp.where(is_core, b, a),
        jnp.where(is_core, a, b),
        jnp.where(is_core, d, c),
        jnp.where(is_core, c, d),
    )
    return (
        jnp.where(is_odd, c, a),
        jnp.where(is_odd, d, b),
        jnp.where(is_odd, a, c),
        jnp.where(is_odd, b, d),
    )


def payload_kernel(tokens_ref, routes_ref, gates_ref, gain_ref, out_ref, meta_ref):
    width = tokens_ref.shape[1]
    per_dev = tokens_ref.shape[0]
    topk = routes_ref.shape[0]
    values = tokens_ref[...].astype(F32)
    mean = jnp.mean(values * values, axis=1, keepdims=True)
    out_ref[:, :width] = (values * lax.rsqrt(mean + EPSILON) * gain_ref[...]).astype(BF16)
    gates = gates_ref[...]
    high = gates.astype(BF16).astype(F32)
    mid = (gates - high).astype(BF16).astype(F32)
    meta_ref[...] = jnp.zeros(meta_ref.shape, F32)
    meta_ref[0:topk, 0:per_dev] = routes_ref[...].astype(F32)
    meta_ref[topk : 2 * topk, 0:per_dev] = high
    meta_ref[2 * topk : 3 * topk, 0:per_dev] = mid
    meta_ref[3 * topk : 4 * topk, 0:per_dev] = gates - high - mid
    out_ref[:, width:] = jnp.transpose(meta_ref[...])[:per_dev, :].astype(BF16)


def shed(load, capacity):
    group = load.shape[0]
    even = lax.broadcasted_iota(jnp.int32, load.shape, 0) % 2 == 0
    at = lambda x, d: pltpu.roll(x, (-d) % group, 0)
    chip = load + jnp.where(even, at(load, 1), at(load, -1))
    half = capacity // 2
    over = jnp.where(chip > capacity, jnp.maximum(load - half, 0.0), 0.0)
    kept = load - over
    settled = jnp.where(even, kept + at(kept, 1) + at(over, -2) + at(over, 3), 0.0)
    return kept, chip, settled


def windows(at_ref, keep_ref, got_ref):
    is_core = at_ref[1] == 1
    chips, cols, slots = keep_ref.shape
    keep = keep_ref[...].astype(F32).reshape(chips * cols, slots)
    got = got_ref[...].astype(F32).reshape(chips * cols, slots)
    return jnp.where(is_core, got, keep), jnp.where(is_core, keep, got)


def spill_kernel(at_ref, keep_ref, got_ref, right_ref, left_ref):
    low, high = windows(at_ref, keep_ref, got_ref)
    rows = right_ref.shape[0]
    side = LANES // 2
    lane = lax.broadcasted_iota(jnp.int32, (rows, LANES), 1)
    right_ref[...] = jnp.where(
        lane >= side, low[:rows], pltpu.roll(low[rows:], side, 1)
    ).astype(BF16)
    left_ref[...] = jnp.where(
        lane < side, high[:rows], pltpu.roll(high[rows:], side, 1)
    ).astype(BF16)


def pooled_pack_kernel(capacity, at_ref, keep_ref, got_ref, right_ref, left_ref, load_ref, out_ref, took_ref):
    low, high = windows(at_ref, keep_ref, got_ref)
    chips, cols, slots = keep_ref.shape
    extra = capacity - slots
    half = capacity // 2
    load = load_ref[...]
    group = load.shape[0]
    kept, _, _ = shed(load, capacity)
    over = load - kept
    row = lax.broadcasted_iota(jnp.int32, load.shape, 0)
    first = at_ref[0] // 2 * 2
    came = pltpu.roll(over, 2, 0) + pltpu.roll(over, group - 3, 0)
    bit = jnp.where((row % 2 == 0) & (came > 0.0), jnp.left_shift(1, row % 32 // 2), 0)
    halves = [jnp.where(row // 32 == h, bit, 0) for h in range(group // 32)]
    for h, half_bits in enumerate(halves):
        took_ref[h] = jnp.max(jnp.sum(half_bits, axis=0, keepdims=True).astype(F32)).astype(jnp.int32)
    one = lambda x, e: jnp.max(jnp.where(row == (e + group) % group, x, 0.0)).astype(jnp.int32)
    kept_low, kept_high = one(kept, first), one(kept, first + 1)
    from_left, from_right = one(over, first - 2), one(over, first + 3)
    lane = lax.broadcasted_iota(jnp.int32, low.shape, 1)
    side = LANES // 2
    unfold = lambda ref: jnp.concatenate(
        [ref[...].astype(F32), pltpu.roll(ref[...].astype(F32), side, 1)], axis=0
    )
    low = jnp.where(lane < kept_low, low, 0.0)
    high = jnp.where(lane >= slots - kept_high, high, 0.0)
    left = unfold(right_ref)
    left = jnp.where((lane >= half) & (lane < half + from_left), left, 0.0)
    right = unfold(left_ref)
    top = slots - 1 - half
    right = jnp.where((lane <= top) & (lane > top - from_right), right, 0.0)
    high = pltpu.roll(high, extra, 1)
    left = pltpu.roll(left, (kept_low - half + slots) % slots, 1)
    right = pltpu.roll(right, (capacity - 1 - kept_high - top + slots) % slots, 1)
    main = low + jnp.where(lane >= extra, high, 0.0)
    main = main + jnp.where(lane >= kept_low, left, 0.0)
    main = main + jnp.where(lane >= extra - kept_high, right, 0.0)
    tail = jnp.where(lane < extra, high, 0.0)
    tail = tail + jnp.where(lane < kept_low, left, 0.0)
    tail = tail + jnp.where(lane < extra - kept_high, right, 0.0)
    store_packed(main, tail, extra, out_ref)


def store_packed(main, tail, extra, out_ref):
    chips, packed, slots = out_ref.shape
    cols = main.shape[0] // chips
    groups = slots // extra
    each = cols // groups
    out_ref[:, :cols, :] = main.reshape(chips, cols, slots).astype(BF16)
    tail = tail.reshape(chips, cols, slots)
    out = tail[:, :each].reshape(chips * each, slots)
    for g in range(1, groups):
        out = out + pltpu.roll(
            tail[:, g * each : (g + 1) * each].reshape(chips * each, slots), g * extra, 1
        )
    out_ref[:, cols:, :] = out.reshape(chips, each, slots).astype(BF16)


def experts_kernel(
    topk, sizes, at_ref, a_ref, b_ref, c_ref, d_ref, wg_hbm, wu_hbm, wd_hbm,
    rank_ref, keep_ref, send_ref, load_ref, level_ref, wg_ref, wu_ref, wd_ref, sems,
):
    copies = []
    for i, (src, dst) in enumerate(((wg_hbm, wg_ref), (wu_hbm, wu_ref), (wd_hbm, wd_ref))):
        step = dst.shape[0] // CHUNKS
        copies.append(
            [
                pltpu.make_async_copy(
                    src.at[0, pl.ds(c * step, step)], dst.at[pl.ds(c * step, step)], sems.at[i, c]
                )
                for c in range(CHUNKS)
            ]
        )
    for copy in sum(copies, []):
        copy.start()
    width = wg_ref.shape[0]
    is_core = at_ref[1] == 1
    is_odd = at_ref[2] == 1
    me = at_ref[0].astype(F32)
    group, total = rank_ref.shape
    chips, cols, slots = keep_ref.shape
    per_dev = total // group
    part = a_ref.shape[0]
    outer = part // per_dev
    refs = (a_ref, b_ref, c_ref, d_ref)
    meta = by_class([r[:, width:].astype(F32) for r in refs], is_core, is_odd)
    grouped = jnp.concatenate([jnp.transpose(m) for m in meta], axis=1)
    rows = jnp.concatenate(
        [m[i * per_dev : (i + 1) * per_dev] for i in range(outer) for m in meta], axis=0
    )
    ordered = jnp.concatenate(
        [jnp.transpose(rows[i * LANES : (i + 1) * LANES]) for i in range(total // LANES)], axis=1
    )
    expert = lax.broadcasted_iota(jnp.int32, (group, total), 0).astype(F32)
    match = jnp.zeros((group, total), F32)
    for k in range(topk):
        match = match + jnp.where(ordered[k : k + 1, :] == expert, 1.0, 0.0)
    index = lax.broadcasted_iota(jnp.int32, (total, total), 0)
    at = lax.broadcasted_iota(jnp.int32, (1, total), 1)
    place = at % part // per_dev * (per_dev * CLASSES) + at // part * per_dev + at % per_dev
    counts = match.astype(BF16)
    rank = jnp.dot(
        counts, jnp.where(index < at, 1.0, 0.0).astype(BF16), preferred_element_type=F32
    )
    rank_ref[...] = jnp.where(match > 0.0, rank, -1.0)
    moved = jnp.dot(
        counts, jnp.where(index < place, 1.0, 0.0).astype(BF16), preferred_element_type=F32
    )
    slot = jnp.sum(jnp.where(expert == me, moved, 0.0), axis=0, keepdims=True)
    slot = jnp.where(is_core, slots - 1 - slot, slot)
    gates = grouped[topk : 2 * topk] + grouped[2 * topk : 3 * topk] + grouped[3 * topk : 4 * topk]
    mine = jnp.zeros((1, total), F32)
    gate = jnp.zeros((1, total), F32)
    for k in range(topk):
        named = grouped[k : k + 1, :] == me
        mine = jnp.where(named, 1.0, mine)
        gate = jnp.where(named, gates[k : k + 1, :], gate)
    slot = jnp.where(mine > 0.0, slot, -1.0).astype(jnp.int32)
    gate = jnp.concatenate(
        by_class([gate[:, k * part : (k + 1) * part] for k in range(CLASSES)], is_core, is_odd), axis=1
    )
    slot = jnp.concatenate(
        by_class([slot[:, k * part : (k + 1) * part] for k in range(CLASSES)], is_core, is_odd), axis=1
    )
    load = jnp.broadcast_to(jnp.sum(match, axis=1, keepdims=True), (group, LANES))
    load_ref[...] = load
    kept, chip, settled = shed(load, sizes[0])
    most = jnp.max(chip).astype(jnp.int32)
    fits = (jnp.max(settled).astype(jnp.int32) <= sizes[0]).astype(jnp.int32)
    level_ref[0] = jnp.where(
        most <= sizes[0], 0, jnp.where(most <= sizes[1], 1, 3 - fits)
    ).astype(jnp.int32)

    hit = lax.broadcasted_iota(jnp.int32, (slots, total), 0) == slot
    pick = jnp.where(hit, 1.0, 0.0).astype(BF16)
    gate = jnp.sum(jnp.where(hit, gate, 0.0), axis=1, keepdims=True)
    picked = jnp.zeros((slots, width), F32)
    for k, ref in enumerate(refs):
        picked = picked + jnp.dot(
            pick[:, k * part : (k + 1) * part], ref[:, :width], preferred_element_type=F32
        )
    picked = picked.astype(BF16)
    for copy in copies[0]:
        copy.wait()
    gate_val = jnp.dot(picked, wg_ref[...], preferred_element_type=F32)
    for copy in copies[1]:
        copy.wait()
    up_val = jnp.dot(picked, wu_ref[...], preferred_element_type=F32)
    act = (gate_val * jax.nn.sigmoid(gate_val) * up_val * gate).astype(BF16)
    for copy in copies[2]:
        copy.wait()
    result = jnp.dot(act, wd_ref[...], preferred_element_type=F32)
    result = jnp.transpose(result).reshape(chips, 2, cols, slots)
    even, odd = result[:, 0], result[:, 1]
    keep_ref[...] = jnp.where(is_core, odd, even).astype(BF16)
    send_ref[...] = jnp.where(is_core, even, odd).astype(BF16)


def pack_kernel(capacity, at_ref, keep_ref, got_ref, out_ref):
    low, high = windows(at_ref, keep_ref, got_ref)
    extra = capacity - keep_ref.shape[2]
    if extra == keep_ref.shape[2]:
        main, tail = low, high
    else:
        high = pltpu.roll(high, extra, 1)
        spill = lax.broadcasted_iota(jnp.int32, high.shape, 1) < extra
        main = low + jnp.where(spill, 0.0, high)
        tail = jnp.where(spill, high, 0.0)
    store_packed(main, tail, extra, out_ref)


def combine_kernel(capacity, pooled, took_ref, rows_ref, rank_ref, load_ref, out_ref, square_ref, kept_ref):
    cols, total = out_ref.shape
    chips = rows_ref.shape[0]
    extra = capacity - LANES
    groups = LANES // extra
    each = cols // groups
    slot = lax.broadcasted_iota(jnp.int32, (capacity, total), 0).astype(F32).astype(BF16)
    col = lax.broadcasted_iota(jnp.int32, (cols, LANES), 0)
    lane = lax.broadcasted_iota(jnp.int32, (cols, LANES), 1)
    own = (col // each) == (lane // extra)
    one = jnp.ones((), BF16)
    zero = jnp.zeros((), BF16)
    group = rank_ref.shape[0]
    half = capacity // 2
    if pooled:
        kept, _, _ = shed(load_ref[...], capacity)
        kept_ref[...] = jnp.concatenate([kept] * (total // LANES), axis=1)

    def add(s, acc, hit):
        pick = jnp.where(hit, one, zero)
        pick = jnp.concatenate([pick[:LANES]] + [pick[LANES:]] * groups, axis=0)
        block = rows_ref[s].astype(F32)
        tail = jnp.concatenate([block[cols:]] * groups, axis=0)
        tail = jnp.where(own, tail, 0.0)
        left = jnp.concatenate([block[:cols], tail], axis=1).astype(BF16)
        return acc + jnp.dot(left, pick, preferred_element_type=F32)

    def keys(s):
        low = rank_ref[pl.ds(2 * s, 1), :]
        high = rank_ref[pl.ds(2 * s + 1, 1), :]
        if pooled:
            low = jnp.where(low < kept_ref[pl.ds(2 * s, 1), :], low, -1.0)
            high = jnp.where(high < kept_ref[pl.ds(2 * s + 1, 1), :], high, -1.0)
        high = jnp.where(high < 0.0, -1.0, capacity - 1.0 - high)
        return (slot == low.astype(BF16)) | (slot == high.astype(BF16))

    def step(i, acc):
        mains, tails, main_picks, tail_picks = [], [], [], []
        for first in range(0, BATCH, groups):
            spread = jnp.zeros((cols, LANES), F32)
            for q in range(groups):
                s = i * BATCH + first + q
                pick = jnp.where(keys(s), one, zero)
                main_picks.append(pick[:LANES])
                tail_picks.append(pick[LANES:])
                block = rows_ref[s].astype(F32)
                mains.append(block[:cols])
                tail = block[cols:]
                turned = [tail] + [pltpu.roll(tail, k * extra, 1) for k in range(1, groups)]
                tail = jnp.concatenate([turned[(q - g) % groups] for g in range(groups)], axis=0)
                spread = jnp.where(lane // extra == q, tail, spread)
            tails.append(spread)
        left = jnp.concatenate(mains + tails, axis=1).astype(BF16)
        pick = jnp.concatenate(main_picks + tail_picks, axis=0)
        return acc + jnp.dot(left, pick, preferred_element_type=F32)

    out = lax.fori_loop(0, chips // BATCH, step, jnp.zeros((cols, total), F32), unroll=2)
    if pooled:

        def more(s, acc):
            def surplus(acc):
                before = lax.rem(2 * s - 2 + group, group)
                after = lax.rem(2 * s + 3, group)
                left = rank_ref[pl.ds(before, 1), :]
                right = rank_ref[pl.ds(after, 1), :]
                left = jnp.where(
                    left < kept_ref[pl.ds(before, 1), :],
                    -1.0,
                    kept_ref[pl.ds(2 * s, 1), :] + left - half,
                )
                right = jnp.where(
                    right < kept_ref[pl.ds(after, 1), :],
                    -1.0,
                    capacity - 1.0 - (kept_ref[pl.ds(2 * s + 1, 1), :] + right - half),
                )
                return add(s, acc, (slot == left.astype(BF16)) | (slot == right.astype(BF16)))

            took = (took_ref[s // 16] >> (s % 16)) & 1
            return lax.cond(took == 1, surplus, lambda acc: acc, acc)

        out = lax.fori_loop(0, chips, more, out)
    out_ref[...] = out
    square_ref[...] = jnp.sum(out * out, axis=0, keepdims=True)


def spread_kernel(mine_ref, other_ref, out_ref):
    square = mine_ref[...] + other_ref[...]
    chips, lines, _ = out_ref.shape
    for i in range(lines):
        out_ref[:, i : i + 1, :] = jnp.broadcast_to(
            square[None, :, i * LANES : (i + 1) * LANES], (chips, 1, LANES)
        ).astype(BF16)


def finish_kernel(width, at_ref, squares_ref, mixed_ref, gain_ref, out_ref):
    sums = jnp.sum(squares_ref[...].astype(F32), axis=0)
    mean = jnp.concatenate([sums[i : i + 1] for i in range(sums.shape[0])], axis=1) / width
    cols = mixed_ref.shape[0]
    each = LANES // cols
    me = at_ref[0]
    gain = jnp.broadcast_to(gain_ref[pl.ds(me // each, 1), :], (LANES, LANES))
    gain = pltpu.roll(gain, (each - me % each) % each * cols, 1)
    gain = jnp.transpose(gain)[:cols, :1]
    out_ref[...] = (mixed_ref[...] * lax.rsqrt(mean + EPSILON) * gain).astype(BF16)


def shards(tokens, routes, gate_weights, norm_gain, final_gain, w_gate, w_up, w_down):
    per_dev, width = tokens.shape
    topk = routes.shape[1]
    group = lax.axis_size(EP)
    chips = group // 2
    cols = width // group
    total = per_dev * group
    most = 2 * group
    me = lax.axis_index(EP)
    core = lax.axis_index("core")
    odd = lax.axis_index("zl")
    at = jnp.stack([me, core, odd]).astype(jnp.int32)

    payload = pl.pallas_call(
        payload_kernel,
        out_shape=jax.ShapeDtypeStruct((per_dev, width + LANES), BF16),
        scratch_shapes=[pltpu.VMEM((LANES, LANES), F32)],
    )(tokens, jnp.transpose(routes), jnp.transpose(gate_weights), norm_gain[None, :])

    zigzag = []
    for chip in range(chips):
        zigzag.append((chip * 2, ((chip + 1) % chips) * 2))
        zigzag.append((chip * 2 + 1, ((chip - 1) % chips) * 2 + 1))
    swap = [(0, 1), (1, 0)]
    own = lax.all_gather(payload, "zh", axis=0, tiled=True)
    near = lax.ppermute(own, EP, zigzag)
    own_pair = lax.ppermute(own, "core", swap)
    near_pair = lax.ppermute(near, "core", swap)
    pieces = (own, own_pair, near, near_pair)
    part = own.shape[0]

    window = jax.ShapeDtypeStruct((chips, cols, LANES), BF16)
    sizes = (most * 5 // 4, most * 3 // 2, most * 2)
    rank, keep, send, load, level = pl.pallas_call(
        functools.partial(experts_kernel, topk, sizes),
        in_specs=[SMEM] + [VMEM] * CLASSES + [HBM] * 3,
        out_specs=[VMEM, VMEM, VMEM, VMEM, SMEM],
        out_shape=[
            jax.ShapeDtypeStruct((group, total), F32),
            window,
            window,
            jax.ShapeDtypeStruct((group, LANES), F32),
            jax.ShapeDtypeStruct((1,), jnp.int32),
        ],
        scratch_shapes=[
            pltpu.VMEM(w_gate.shape[1:], BF16),
            pltpu.VMEM(w_up.shape[1:], BF16),
            pltpu.VMEM(w_down.shape[1:], BF16),
            pltpu.SemaphoreType.DMA((3, CHUNKS)),
        ],
        compiler_params=pltpu.CompilerParams(vmem_limit_bytes=50 << 20),
    )(at, *pieces, w_gate, w_up, w_down)
    got = lax.ppermute(send, "core", swap)
    lines = total // LANES

    right = [(i, (i + 2) % group) for i in range(group)]
    left = [(i, (i - 2) % group) for i in range(group)]
    small = pltpu.CompilerParams(vmem_limit_bytes=16 << 20)

    def branch(capacity, pooled):
        packed = cols * capacity // LANES
        message = jax.ShapeDtypeStruct((chips, packed, LANES), BF16)
        spill = jax.ShapeDtypeStruct((chips * cols // 2, LANES), BF16)

        def run(at, keep, got, rank, load):
            if pooled:
                to_right, to_left = pl.pallas_call(
                    spill_kernel,
                    in_specs=[SMEM, VMEM, VMEM],
                    out_shape=[spill, spill],
                    compiler_params=small,
                )(at, keep, got)
                both, took = pl.pallas_call(
                    functools.partial(pooled_pack_kernel, capacity),
                    in_specs=[SMEM] + [VMEM] * 5,
                    out_specs=[VMEM, SMEM],
                    out_shape=[message, jax.ShapeDtypeStruct((group // 32,), jnp.int32)],
                    compiler_params=small,
                )(at, keep, got, lax.ppermute(to_right, EP, right), lax.ppermute(to_left, EP, left), load)
            else:
                took = at
                both = pl.pallas_call(
                    functools.partial(pack_kernel, capacity),
                    in_specs=[SMEM, VMEM, VMEM],
                    out_shape=message,
                    compiler_params=small,
                )(at, keep, got)
            returned = lax.all_to_all(both, CHIPS, split_axis=0, concat_axis=0, tiled=True)
            return pl.pallas_call(
                functools.partial(combine_kernel, capacity, pooled),
                in_specs=[SMEM] + [VMEM] * 3,
                out_shape=[
                    jax.ShapeDtypeStruct((cols, total), F32),
                    jax.ShapeDtypeStruct((1, total), F32),
                ],
                scratch_shapes=[pltpu.VMEM((group, total), F32)],
                compiler_params=small,
            )(took, returned, rank, load)

        return run

    mixed, square = lax.switch(
        level[0],
        [branch(sizes[0], False), branch(sizes[1], False), branch(sizes[0], True), branch(sizes[2], False)],
        at, keep, got, rank, load,
    )

    spread = pl.pallas_call(
        spread_kernel,
        in_specs=[VMEM] * 2,
        out_shape=jax.ShapeDtypeStruct((chips, total // LANES, LANES), BF16),
        compiler_params=small,
    )(square, lax.ppermute(square, "core", swap))
    squares = lax.all_to_all(spread, CHIPS, split_axis=0, concat_axis=0, tiled=True)
    finished = pl.pallas_call(
        functools.partial(finish_kernel, width),
        in_specs=[SMEM] + [VMEM] * 3,
        out_shape=jax.ShapeDtypeStruct((cols, total), BF16),
        compiler_params=small,
    )(at, squares, mixed, final_gain.reshape(-1, LANES))
    return jnp.transpose(finished)


def solution(mesh):
    split = Mesh(mesh.devices.reshape(mesh.shape["grp"], 16, 2, 2), GRP_EP)
    return jax.shard_map(
        shards,
        mesh=split,
        in_specs=(
            P(GRP_EP, None),
            P(GRP_EP, None),
            P(GRP_EP, None),
            P(),
            P(),
            P(EP, None, None),
            P(EP, None, None),
            P(EP, None, None),
        ),
        out_specs=P("grp", EP),
        check_vma=False,
    )
```
